256 devices in a mesh: sp: 32 (over z, x), tp: 4 (over y), dp: 2 (over core).
Axes of the slice: x: 4, y: 4, z: 8, core: 2. Of those that a mesh axis runs over, the one named last changes fastest.
Arguments:
- latent: bfloat16 [4, 32768, 2048], P('dp', 'sp'), may hold values from -6 to 6
- context: bfloat16 [4, 1024, 2048], P('dp', 'sp'), may hold values from -6 to 6
- condition: bfloat16 [4, 2048], P('dp', 'sp'), may hold values from -6 to 6
- ctx_cond: bfloat16 [2048], P('sp'), may hold values from -6 to 6
- norm_gain: float32 [2048], replicated, may hold values from 0.1 to 1.9
- w_shift: bfloat16 [2048, 2048], P('sp', 'tp'), may hold values from -0.125 to 0.125
- w_scale: bfloat16 [2048, 2048], P('sp', 'tp'), may hold values from -0.125 to 0.125
- w_gate: bfloat16 [2048, 2048], P('sp', 'tp'), may hold values from -0.125 to 0.125
- w_query: bfloat16 [2048, 1024], P(None, 'tp'), may hold values from -0.125 to 0.125
- w_key: bfloat16 [2048, 256], P(None, 'tp'), may hold values from -0.125 to 0.125
- w_value: bfloat16 [2048, 256], P(None, 'tp'), may hold values from -0.125 to 0.125
- w_out: bfloat16 [1024, 2048], P('tp'), may hold values from -4 to 4
- sink_logit: float32 [16], P('tp'), may hold values from 4 to 7
- ctx_lift: float32 [16], P('tp'), may hold values from -4 to 220
Outputs:
- mixed: bfloat16 [4, 32768, 2048], P('dp', ('sp', 'tp'))
The draws below stay inside these ranges and needn't reach their ends.
All inputs are finite; a program needn't handle non-finite values.
Results may differ from the reference program's by a relative error of at most 0.012.
Values may be sent and summed in bfloat16 or wider, within the bound.
A program may use at most 128 MiB of HBM per device.

```python
import jax
import jax.numpy as jnp
from jax import lax

D = 2048
HEADS = 16
KV_HEADS = 4
HEAD = 64
WINDOW = 128
GRID_COLS = 64
TOK_DEV = 1024
CTX = 1024
SAMPLES = 4
LATENT = 32768


def draw_ctx_lift(key, part):
    first_key = jax.random.fold_in(key, 11)
    lifted = jax.random.uniform(first_key, (HEADS,), jnp.float32, -3.6, -1.8)
    return lifted


def level_of(own_key, dims, cuts, smallest, largest):
    factor_of = 1.0
    for position, blocks in cuts:
        steps = jax.random.uniform(jax.random.fold_in(jax.random.fold_in(own_key, 6), position), (blocks,), jnp.float32, smallest / len(cuts), largest / len(cuts))
        factor_of = factor_of * jnp.repeat(jnp.exp(steps), dims[position] // blocks).reshape((-1,) + (1,) * (len(dims) - 1 - position))
    return factor_of


def centred(stream_key, shape, deviation, limit, cuts=(), kind=jnp.bfloat16):
    level = level_of(stream_key, shape, cuts, -0.22, 0.18) if cuts else 1.0
    array = jax.random.normal(stream_key, shape, jnp.float32) * deviation * level
    return jnp.minimum(jnp.maximum(array, -limit), limit).astype(kind)


def setup_inputs(seed: int = 0) -> dict:
    splits = jax.random.split(jax.random.key(seed), 15)
    return {
        "latent": centred(splits[0], (SAMPLES, LATENT, D), 1.0, 6.0, ((0, 2), (1, 32))),
        "context": centred(splits[1], (SAMPLES, CTX, D), 1.0, 6.0, ((0, 2), (1, 32))),
        "condition": centred(splits[2], (SAMPLES, D), 1.0, 6.0, ((0, 2), (1, 32))),
        "ctx_cond": centred(splits[3], (D,), 1.0, 6.0, ((0, 32),)),
        "norm_gain": jnp.clip(1.0 + 0.18 * jax.random.normal(splits[4], (D,), jnp.float32), 0.1, 1.9),
        "w_shift": centred(splits[5], (D, D), D ** -0.5, 0.125, ((0, 32), (1, 4))),
        "w_scale": centred(splits[6], (D, D), D ** -0.5, 0.125, ((0, 32), (1, 4))),
        "w_gate": centred(splits[7], (D, D), D ** -0.5, 0.125, ((0, 32), (1, 4))),
        "w_query": centred(splits[8], (D, HEADS * HEAD), D ** -0.5, 0.125, ((1, 4),)),
        "w_key": centred(splits[9], (D, KV_HEADS * HEAD), D ** -0.5, 0.125, ((1, 4),)),
        "w_value": centred(splits[10], (D, KV_HEADS * HEAD), D ** -0.5, 0.125, ((1, 4),)),
        "w_out": centred(splits[11], (HEADS * HEAD, D), 2 ** -0.5, 4.0, ((0, 4),)),
        "sink_logit": jnp.clip(4.0 + 3.0 * jax.random.uniform(splits[12], (HEADS,), jnp.float32) ** level_of(splits[12], (HEADS,), ((0, 4),), -0.2, 0.2), 4.0, 7.0),
        "ctx_lift": draw_ctx_lift(jax.random.fold_in(splits[14], 71), 0),
    }


epsilon = 1e-06
rope_base = 10000.0
masked_value = -1e+30

def modulated(inputs, norm_gain, shift_vec, scale_vec):
    widened = inputs.astype(jnp.float32)
    inverse = lax.rsqrt(lax.optimization_barrier(jnp.mean(widened * widened, axis=-1, keepdims=True)) + epsilon)
    return (widened * inverse * norm_gain * (1.0 + scale_vec) + shift_vec).astype(jnp.bfloat16)

def rotate_half(half_part, angles):
    first_half, second = jnp.split(half_part, 2, axis=-1)
    cosine = jnp.cos(angles)[:, None, :]
    sine_part = jnp.sin(angles)[:, None, :]
    return jnp.concatenate([first_half * cosine - second * sine_part, first_half * sine_part + second * cosine], axis=-1)

def rotate(inputs, positions):
    quarter = inputs.shape[-1] // 4
    frequency = rope_base ** (-jnp.arange(quarter, dtype=jnp.float32) / quarter)
    row_angle = (positions // GRID_COLS).astype(jnp.float32)[:, None] * frequency
    col_angle = (positions % GRID_COLS).astype(jnp.float32)[:, None] * frequency
    half_size = 2 * quarter
    return jnp.concatenate([rotate_half(inputs[..., :half_size], row_angle), rotate_half(inputs[..., half_size:], col_angle)], axis=-1)

def reference(latent, context, condition, ctx_cond, norm_gain, w_shift, w_scale, w_gate, w_query, w_key, w_value, w_out, sink_logit, ctx_lift):
    samples, latent_len, model_width = latent.shape
    cond_rows = jnp.concatenate([condition, ctx_cond[None, :]], axis=0)
    active = jax.nn.silu(cond_rows.astype(jnp.float32)).astype(jnp.bfloat16)
    shift_vec = jnp.dot(active, w_shift, preferred_element_type=jnp.float32)
    scale_vec = jnp.dot(active, w_scale, preferred_element_type=jnp.float32)
    gate_vec = jnp.dot(active, w_gate, preferred_element_type=jnp.float32)
    hidden = modulated(latent, norm_gain, shift_vec[:samples, None, :], scale_vec[:samples, None, :])
    ctx_hidden = modulated(context, norm_gain, shift_vec[samples], scale_vec[samples])
    positions = jnp.arange(latent_len, dtype=jnp.int32)
    flat = hidden.reshape(-1, model_width)
    queries = rotate(jnp.dot(flat, w_query, preferred_element_type=jnp.float32).reshape(samples, latent_len, HEADS, HEAD), positions).astype(jnp.bfloat16)
    key_rows = rotate(jnp.dot(flat, w_key, preferred_element_type=jnp.float32).reshape(samples, latent_len, KV_HEADS, HEAD), positions).astype(jnp.bfloat16)
    values = jnp.dot(flat, w_value, preferred_element_type=jnp.float32).astype(jnp.bfloat16).reshape(samples, latent_len, KV_HEADS, HEAD)
    ctx_flat = ctx_hidden.reshape(-1, model_width)
    ctx_keys = jnp.dot(ctx_flat, w_key, preferred_element_type=jnp.float32).astype(jnp.bfloat16).reshape(samples, CTX, KV_HEADS, HEAD)
    ctx_values = jnp.dot(ctx_flat, w_value, preferred_element_type=jnp.float32).astype(jnp.bfloat16).reshape(samples, CTX, KV_HEADS, HEAD)
    padding = ((0, 0), (WINDOW, WINDOW), (0, 0), (0, 0))
    key_pad = jnp.pad(key_rows, padding)
    value_pad = jnp.pad(values, padding)
    block_rows = min(512, TOK_DEV)
    blocks = latent_len // block_rows
    span_rows = block_rows + 2 * WINDOW
    group_size = HEADS // KV_HEADS
    lift_rows = ctx_lift.astype(jnp.float32).reshape(KV_HEADS, group_size, 1, 1)
    sink_rows = sink_logit.astype(jnp.float32).reshape(KV_HEADS, group_size, 1, 1)
    factor = HEAD ** (-0.5)

    def attend(step_id):
        sample = step_id // blocks
        row_start = step_id % blocks * block_rows
        q_rows = lax.dynamic_slice_in_dim(lax.dynamic_index_in_dim(queries, sample, 0, keepdims=False), row_start, block_rows, 0)
        q_rows = q_rows.reshape(block_rows, KV_HEADS, group_size, HEAD).astype(jnp.float32)
        near_keys = lax.dynamic_slice_in_dim(lax.dynamic_index_in_dim(key_pad, sample, 0, keepdims=False), row_start, span_rows, 0).astype(jnp.float32)
        near_values = lax.dynamic_slice_in_dim(lax.dynamic_index_in_dim(value_pad, sample, 0, keepdims=False), row_start, span_rows, 0).astype(jnp.float32)
        far_keys = lax.dynamic_index_in_dim(ctx_keys, sample, 0, keepdims=False).astype(jnp.float32)
        far_values = lax.dynamic_index_in_dim(ctx_values, sample, 0, keepdims=False).astype(jnp.float32)
        query_pos = row_start + jnp.arange(block_rows, dtype=jnp.int32)
        key_pos = row_start - WINDOW + jnp.arange(span_rows, dtype=jnp.int32)
        inside = (key_pos[None, :] >= 0) & (key_pos[None, :] < latent_len) & (jnp.abs(query_pos[:, None] - key_pos[None, :]) <= WINDOW)
        near_scores = jnp.einsum('qgrd,kgd->grqk', q_rows, near_keys) * factor
        near_scores = jnp.where(inside[None, None], near_scores, masked_value)
        far_scores = jnp.einsum('qgrd,kgd->grqk', q_rows, far_keys) * factor + lift_rows
        row_max = jnp.maximum(jnp.maximum(near_scores.max(-1, keepdims=True), far_scores.max(-1, keepdims=True)), sink_rows)
        near_exp = jnp.exp(near_scores - row_max)
        far_exp = jnp.exp(far_scores - row_max)
        normaliser = near_exp.sum(-1, keepdims=True) + far_exp.sum(-1, keepdims=True) + jnp.exp(sink_rows - row_max)
        near_weights = (near_exp / normaliser).astype(jnp.bfloat16).astype(jnp.float32)
        far_weights = (far_exp / normaliser).astype(jnp.bfloat16).astype(jnp.float32)
        outcome = jnp.einsum('grqk,kgd->qgrd', near_weights, near_values) + jnp.einsum('grqk,kgd->qgrd', far_weights, far_values)
        return outcome.astype(jnp.bfloat16).reshape(block_rows, HEADS * HEAD)
    attended = lax.map(attend, jnp.arange(samples * blocks, dtype=jnp.int32)).reshape(samples, latent_len, HEADS * HEAD)
    projected = jnp.dot(attended.reshape(-1, HEADS * HEAD), w_out, preferred_element_type=jnp.float32).reshape(samples, latent_len, model_width)
    return (gate_vec[:samples, None, :] * projected).astype(jnp.bfloat16)
```

```python
import functools
import math

import jax
import jax.numpy as jnp
from jax import lax
from jax.experimental import pallas as pl
from jax.experimental.pallas import tpu as pltpu
from jax.sharding import PartitionSpec as P

HEAD = 64
WINDOW = 128
GRID_COLS = 64
EPSILON = 1e-06
ROPE_BASE = 10000.0
NEGATIVE = -1e30
LOG2E = math.log2(math.e)
LANES = 128
MESH = pl.DeviceIdType.MESH
f32 = jnp.float32
bf16 = jnp.bfloat16


def lanes_of(rows):
    return lax.broadcasted_iota(jnp.int32, (rows, LANES), 1)


def drain(ref, sem):
    pltpu.make_async_copy(ref, ref, sem).wait()


def swapped(u, lane):
    return jnp.where(lane % 32 < 16, pltpu.roll(u, LANES - 16, 1), pltpu.roll(u, 16, 1))


def prepare(pairs, kt_ref, v4_ref, sample, start, rows):
    wide = pairs.astype(f32)
    turned = pltpu.roll(wide, HEAD, 1)
    low = lanes_of(rows) < HEAD
    kt_ref[sample, :, pl.ds(start, rows)] = jnp.where(low, wide, turned).astype(bf16).T
    v4_ref[sample, pl.ds(start, rows), :LANES] = jnp.where(low, turned, 1.0).astype(bf16)
    v4_ref[sample, pl.ds(start, rows), LANES:] = jnp.where(low, 1.0, wide).astype(bf16)


def attend(sample, row, near_start, left_off, right_off, qp_ref, kt_ref, v4_ref, lift_ref, sink_ref, att_ref, ctx):
    rows = WINDOW
    q = jnp.concatenate([qp_ref[sample, h, pl.ds(row, rows), :] for h in range(4)], axis=0)
    far_keys = kt_ref[sample, :, :ctx]
    near_keys = kt_ref[sample, :, pl.ds(near_start, 3 * WINDOW)]
    far_all = jnp.dot(q, far_keys, preferred_element_type=f32)
    near_all = jnp.dot(q, near_keys, preferred_element_type=f32)
    qi = lax.broadcasted_iota(jnp.int32, (rows, WINDOW), 0)
    kj = lax.broadcasted_iota(jnp.int32, (rows, WINDOW), 1)
    low = lanes_of(rows) < HEAD
    results = []
    for h in range(4):
        lift = lift_ref[h] * LOG2E
        sink = sink_ref[h] * LOG2E
        part = slice(h * rows, (h + 1) * rows)
        far = far_all[part]
        first = jnp.where(kj >= qi, near_all[part, :WINDOW], NEGATIVE) + left_off
        middle = near_all[part, WINDOW : 2 * WINDOW]
        last = jnp.where(kj <= qi, near_all[part, 2 * WINDOW :], NEGATIVE) + right_off
        near_top = jnp.maximum(jnp.maximum(first, middle), last)
        far_top = jnp.max(far, axis=1, keepdims=True) + lift
        top = jnp.maximum(jnp.maximum(jnp.max(near_top, axis=1, keepdims=True), far_top), sink)
        far_exp = jnp.exp2(far - (top - lift)).astype(bf16)
        near_exp = jnp.concatenate(
            [jnp.exp2(first - top), jnp.exp2(middle - top), jnp.exp2(last - top)], axis=1
        ).astype(bf16)
        cols = slice(0, LANES) if h % 2 == 0 else slice(LANES, 2 * LANES)
        total = jnp.dot(far_exp, v4_ref[sample, :ctx, cols], preferred_element_type=f32) + jnp.dot(
            near_exp, v4_ref[sample, pl.ds(near_start, 3 * WINDOW), cols], preferred_element_type=f32
        )
        weight = pltpu.roll(total, HEAD, 1) + jnp.exp2(sink - top)
        results.append(total / weight)
    for pair in range(2):
        att_ref[sample, pl.ds(row, rows), pair * LANES : (pair + 1) * LANES] = jnp.where(
            low, results[2 * pair], results[2 * pair + 1]
        ).astype(bf16)


def layer(
    sizes,
    x_hbm, context_hbm, condition, ctx_cond, gain, wsh_hbm, wsc_hbm, wga_hbm, wq_hbm, wk_hbm, wv_hbm, wo_hbm,
    sink_ref, lift_ref,
    out_hbm,
    x_v, context_v, wm_v, wq_v, wk_v, wv_v, wkv_v, wo_v,
    active_v, part_v, rx_v, zsrc_v, rz_v, mod_v, modr_v, mul_v, add_v,
    inv_v, cos_v, sin_v, qp_v, kv_v, ckv_v, kt_v, v4_v, att_v, by_v, out_v,
    local_sem, stage_sem, halo_send, halo_recv, wo_send, wo_recv, att_send, att_recv,
):
    nsp, nx, nt, nd = sizes
    nz = nsp // nx
    samples, tokens, width = x_v.shape
    chunk = tokens // nt
    ctx_local = context_v.shape[1]
    ctx = ctx_local * nsp
    sp = lax.axis_index("sp")
    tp = lax.axis_index("tp")
    dp = lax.axis_index("dp")
    xi = lax.rem(sp, nx)
    zi = lax.div(sp, nx)

    def place(sp_to=None, tp_to=None, dp_to=None):
        return {
            "sp": sp if sp_to is None else sp_to,
            "tp": tp if tp_to is None else tp_to,
            "dp": dp if dp_to is None else dp_to,
        }

    def remote(src, dst, send, recv, device):
        return pltpu.make_async_remote_copy(
            src_ref=src, dst_ref=dst, send_sem=send, recv_sem=recv, device_id=device, device_id_type=MESH
        )

    def x_peer(offset):
        return zi * nx + lax.rem(xi + offset, nx)

    def z_peer(offset):
        return lax.rem(zi + offset, nz) * nx + xi

    own_rows = wo_hbm.shape[0]
    half = own_rows // nd
    loads = [
        pltpu.make_async_copy(wsh_hbm, wm_v.at[0], local_sem.at[0]),
        pltpu.make_async_copy(wsc_hbm, wm_v.at[1], local_sem.at[1]),
        pltpu.make_async_copy(wga_hbm, wm_v.at[2], local_sem.at[2]),
        pltpu.make_async_copy(
            wo_hbm, wo_v.at[pl.ds(pl.multiple_of(tp * own_rows, own_rows), own_rows), :], local_sem.at[3]
        ),
        pltpu.make_async_copy(context_hbm, context_v, local_sem.at[4]),
        pltpu.make_async_copy(x_hbm, x_v, local_sem.at[5]),
        pltpu.make_async_copy(wk_hbm, wk_v, local_sem.at[6]),
        pltpu.make_async_copy(wv_hbm, wv_v, local_sem.at[7]),
        pltpu.make_async_copy(wq_hbm, wq_v, local_sem.at[8]),
    ]
    for load in loads:
        load.start()

    barrier = pltpu.get_barrier_semaphore()

    def greet(device):
        pl.semaphore_signal(barrier, inc=1, device_id=device, device_id_type=MESH)

    for offset in range(1, nsp):
        greet(place(sp_to=lax.rem(sp + offset, nsp)))
    for dy in range(1, nt):
        for dx in range(nx):
            greet(place(sp_to=x_peer(dx), tp_to=lax.rem(tp + dy, nt)))
    for offset in range(1, nd):
        greet(place(dp_to=lax.rem(dp + offset, nd)))

    active_v[...] = jnp.zeros_like(active_v)
    active_v[0:2, :] = condition[...].astype(f32)
    active_v[2:3, :] = ctx_cond[...].astype(f32)
    raw = active_v[...]
    active = (raw / (1.0 + jnp.exp(-raw))).astype(bf16)
    for load in loads[:3]:
        load.wait()
    vecs = [jnp.dot(active, wm_v[k], preferred_element_type=f32) for k in range(3)]
    for c in range(nx):
        cols = slice(c * LANES, (c + 1) * LANES)
        part_v[c, 0:3, :] = vecs[0][0:3, cols]
        part_v[c, 3:6, :] = vecs[1][0:3, cols]
        part_v[c, 6:8, :] = vecs[2][0:2, cols]

    pl.semaphore_wait(barrier, (nsp - 1) + (nt - 1) * nx + (nd - 1))

    for offset in range(1, nx):
        to = lax.rem(xi + offset, nx)
        remote(part_v.at[to], rx_v.at[offset - 1], stage_sem.at[0], stage_sem.at[1], place(sp_to=x_peer(offset))).start()

    loads[3].wait()

    def wo_rows(owner, core, start, count):
        return wo_v.at[pl.ds(pl.multiple_of(owner * own_rows + core * half + start, count), count), :]

    after = lax.rem(tp + 1, nt)
    before = lax.rem(tp + nt - 1, nt)
    across = lax.rem(tp + 2, nt)
    other = lax.rem(dp + 1, nd)
    quarter = half // 2

    def wo_copy(k, ref, device):
        return remote(ref, ref, wo_send.at[k], wo_recv.at[k], device)

    mine = wo_rows(tp, dp, 0, half)
    to_after = wo_copy(0, mine, place(tp_to=after))
    to_before = wo_copy(1, mine, place(tp_to=before))
    to_after.start()
    to_before.start()

    block = min(256, chunk)
    blocks = tokens // block

    def statistics(step):
        sample, start = step // blocks, pl.multiple_of(step % blocks * block, block)
        total = jnp.zeros((block, LANES), f32)
        for c in range(width // LANES):
            piece = x_v[sample, pl.ds(start, block), c * LANES : (c + 1) * LANES].astype(f32)
            total = total + piece * piece
        mean = jnp.sum(total, axis=1, keepdims=True) / width
        inv_v[sample, pl.ds(start, block), :] = jnp.broadcast_to(lax.rsqrt(mean + EPSILON), (block, LANES))

    low_wide = lanes_of(width) < HEAD
    loads[6].wait()
    loads[7].wait()
    wkv_v[...] = jnp.concatenate([wk_v[...], wv_v[...]], axis=1)
    loads[5].wait()

    def stats_loop(first, last):
        def run(step, carry):
            statistics(step)
            return carry

        lax.fori_loop(first, last, run, 0)

    all_blocks = samples * blocks
    stats_loop(0, all_blocks // 2)

    drain(rx_v, stage_sem.at[1])
    quarter_sum = part_v[xi]
    for k in range(nx - 1):
        quarter_sum = quarter_sum + rx_v[k]
    zsrc_v[...] = quarter_sum

    for offset in range(1, nz):
        remote(zsrc_v, rz_v.at[offset - 1], stage_sem.at[2], stage_sem.at[3], place(sp_to=z_peer(offset))).start()

    stats_loop(all_blocks // 2, all_blocks)
    lane1 = lanes_of(8)
    frequency = jnp.exp((lane1[0:1] % 16).astype(f32) * (-math.log(ROPE_BASE) / 16.0))
    grid_rows = tokens // GRID_COLS
    table_rows = max(grid_rows, 8)
    row_pos = (sp * grid_rows + lax.broadcasted_iota(jnp.int32, (table_rows, LANES), 0)).astype(f32)
    col_pos = lax.broadcasted_iota(jnp.int32, (GRID_COLS, LANES), 0).astype(f32)
    row_cos, row_sin = jnp.cos(row_pos * frequency), jnp.sin(row_pos * frequency)
    col_cos, col_sin = jnp.cos(col_pos * frequency), jnp.sin(col_pos * frequency)
    lane64 = lanes_of(GRID_COLS)
    by_row = lane64 % HEAD < 32
    minus = lane64 % 32 < 16
    for t in range(grid_rows):
        rows = slice(t * GRID_COLS, (t + 1) * GRID_COLS)
        cos_v[rows, :] = jnp.where(by_row, row_cos[t : t + 1, :], col_cos)
        sine = jnp.where(by_row, row_sin[t : t + 1, :], col_sin)
        sin_v[rows, :] = jnp.where(minus, -sine, sine)

    drain(rz_v, stage_sem.at[3])
    total = zsrc_v[...]
    for k in range(nz - 1):
        total = total + rz_v[k]
    here = tp * nx + xi
    mod_v[here] = total

    for dy in range(nt):
        for dx in range(nx):
            if dy or dx:
                remote(
                    mod_v.at[here], mod_v.at[here], stage_sem.at[4], stage_sem.at[5],
                    place(sp_to=x_peer(dx), tp_to=lax.rem(tp + dy, nt)),
                ).start()

    @pl.when(sp == 0)
    def _():
        kv_v[:, 0:WINDOW, :] = jnp.zeros((samples, WINDOW, LANES), bf16)

    @pl.when(sp == nsp - 1)
    def _():
        kv_v[:, WINDOW + tokens :, :] = jnp.zeros((samples, WINDOW, LANES), bf16)

    loads[4].wait()
    loads[8].wait()
    ctx_rows = samples * ctx_local
    ctx_wide = context_v[...].reshape(ctx_rows, width).astype(f32)
    ctx_inv = lax.rsqrt(jnp.mean(ctx_wide * ctx_wide, axis=1, keepdims=True) + EPSILON)
    ctx_unit = ctx_wide * ctx_inv

    drain(mod_v.at[pl.ds(0, nt * nx - 1)], stage_sem.at[5])
    for k in range(nt * nx):
        modr_v[:, k * LANES : (k + 1) * LANES] = mod_v[k]
    scaled = gain[...] * (1.0 + modr_v[3:6, :])
    for r in range(samples):
        mul_v[r, 0:1, :] = scaled[r : r + 1]
        add_v[r, 0:1, :] = modr_v[r : r + 1, :]

    ctx_hidden = (ctx_unit * scaled[2:3] + modr_v[2:3, :]).astype(bf16)
    ctx_pairs = jnp.dot(ctx_hidden, wkv_v[...], preferred_element_type=f32).astype(bf16)
    ckv_v[sp] = ctx_pairs.reshape(samples, ctx_local, LANES)
    for offset in range(1, nsp):
        remote(
            ckv_v.at[sp], ckv_v.at[sp], stage_sem.at[6], stage_sem.at[7], place(sp_to=lax.rem(sp + offset, nsp))
        ).start()

    from_before = wo_rows(before, dp, 0, half)
    from_after = wo_rows(after, dp, 0, half)
    wo_copy(0, from_before, place(tp_to=after)).wait_recv()
    on_after = wo_copy(2, wo_rows(before, dp, 0, quarter), place(tp_to=after))
    on_after.start()
    wo_copy(1, from_after, place(tp_to=before)).wait_recv()
    on_before = wo_copy(3, wo_rows(after, dp, quarter, quarter), place(tp_to=before))
    on_before.start()
    over_before = wo_copy(4, from_before, place(dp_to=other))
    over_after = wo_copy(5, from_after, place(dp_to=other))
    over_before.start()
    over_after.start()

    lane = lanes_of(block)
    low = lane < HEAD

    def project(sample, index):
        start = pl.multiple_of(index * block, block)
        inverse = inv_v[sample, pl.ds(start, block), :]
        steps = 4
        deep = width // steps
        q_acc = jnp.zeros((block, 2 * LANES), f32)
        kv_acc = jnp.zeros((block, LANES), f32)
        for k in range(steps):
            pieces = []
            for c in range(deep // LANES):
                cols = slice(k * deep + c * LANES, k * deep + (c + 1) * LANES)
                wide = x_v[sample, pl.ds(start, block), cols].astype(f32)
                pieces.append(
                    (wide * inverse * mul_v[sample, 0:1, cols] + add_v[sample, 0:1, cols]).astype(bf16)
                )
            hidden = jnp.concatenate(pieces, axis=1)
            q_acc = q_acc + jnp.dot(hidden, wq_v[k * deep : (k + 1) * deep, :], preferred_element_type=f32)
            kv_acc = kv_acc + jnp.dot(hidden, wkv_v[k * deep : (k + 1) * deep, :], preferred_element_type=f32)
        cosine = cos_v[pl.ds(start, block), :]
        sine = sin_v[pl.ds(start, block), :]
        turned = kv_acc * cosine + swapped(kv_acc, lane) * sine
        kv_v[sample, pl.ds(pl.multiple_of(WINDOW + start, WINDOW), block), :] = jnp.where(low, turned, kv_acc).astype(bf16)
        factor = HEAD ** (-0.5) * LOG2E
        for pair in range(2):
            u = q_acc[:, pair * LANES : (pair + 1) * LANES]
            turned = (u * cosine + swapped(u, lane) * sine) * factor
            qp_v[sample, 2 * pair, pl.ds(start, block), :] = jnp.where(low, turned, 0.0).astype(bf16)
            qp_v[sample, 2 * pair + 1, pl.ds(start, block), :] = jnp.where(low, 0.0, turned).astype(bf16)

    def edges(step, carry):
        project(step // 2, step % 2 * (blocks - 1))
        return carry

    lax.fori_loop(0, 2 * samples, edges, 0)

    send_right = remote(
        kv_v.at[:, pl.ds(tokens, WINDOW), :], kv_v.at[:, pl.ds(0, WINDOW), :], halo_send.at[0], halo_recv.at[0],
        place(sp_to=lax.rem(sp + 1, nsp)),
    )
    send_left = remote(
        kv_v.at[:, pl.ds(WINDOW, WINDOW), :], kv_v.at[:, pl.ds(WINDOW + tokens, WINDOW), :], halo_send.at[1],
        halo_recv.at[1], place(sp_to=lax.rem(sp + nsp - 1, nsp)),
    )

    @pl.when(sp < nsp - 1)
    def _():
        send_right.start()

    @pl.when(sp > 0)
    def _():
        send_left.start()

    inner = blocks - 2

    def middles(step, carry):
        project(step // inner, 1 + step % inner)
        return carry

    lax.fori_loop(0, inner * samples, middles, 0)

    from_across = wo_rows(across, dp, 0, half)
    wo_copy(2, wo_rows(across, dp, 0, quarter), place(tp_to=after)).wait_recv()
    wo_copy(3, wo_rows(across, dp, quarter, quarter), place(tp_to=before)).wait_recv()
    over_across = wo_copy(6, from_across, place(dp_to=other))
    over_across.start()

    @pl.when(sp > 0)
    def _():
        send_right.wait_recv()

    @pl.when(sp < nsp - 1)
    def _():
        send_left.wait_recv()

    for sample in range(samples):
        prepare(kv_v[sample], kt_v, v4_v, sample, ctx, tokens + 2 * WINDOW)
    drain(ckv_v.at[pl.ds(0, nsp - 1)], stage_sem.at[7])
    for sample in range(samples):
        prepare(ckv_v[:, sample].reshape(ctx, LANES), kt_v, v4_v, sample, 0, ctx)

    def att_copy(step_k, sample, dest):
        return remote(
            att_v.at[sample, pl.ds(pl.multiple_of(dest * chunk, chunk), chunk), :], by_v.at[tp, sample],
            att_send.at[step_k, sample], att_recv.at[step_k, sample], place(tp_to=dest),
        )

    def chunk_step(step, carry):
        k, sample = step // samples, step % samples
        dest = lax.rem(tp + 1 + k, nt)
        for sub in range(chunk // WINDOW):
            row = pl.multiple_of(dest * chunk + sub * WINDOW, WINDOW)
            left_off = jnp.where((sp == 0) & (row == 0), NEGATIVE, 0.0)
            right_off = jnp.where((sp == nsp - 1) & (row == tokens - WINDOW), NEGATIVE, 0.0)
            attend(
                sample, row, pl.multiple_of(ctx + row, WINDOW), left_off, right_off, qp_v, kt_v, v4_v, lift_ref,
                sink_ref, att_v, ctx,
            )

        @pl.when(k < nt - 1)
        def _():
            att_copy(k, sample, dest).start()

        return carry

    lax.fori_loop(0, nt * samples, chunk_step, 0)
    by_v[tp] = att_v[:, pl.ds(pl.multiple_of(tp * chunk, chunk), chunk), :]

    for k in (4, 5, 6):
        wo_copy(k, wo_rows(tp, dp, 0, half), place(dp_to=other)).wait_recv()
    for k in range(nt - 1):
        for sample in range(samples):
            att_copy(k, sample, lax.rem(tp + 1 + k, nt)).wait_recv()

    wide = 512
    for sample in range(samples):

        def project_out(step, carry):
            cols = pl.ds(pl.multiple_of(step * wide, wide), wide)
            total = jnp.zeros((chunk, wide), f32)
            for t in range(nt):
                total = total + jnp.dot(
                    by_v[t, sample], wo_v[t * own_rows : (t + 1) * own_rows, cols], preferred_element_type=f32
                )
            out_v[sample, :, cols] = (total * modr_v[6 + sample : 7 + sample, cols]).astype(bf16)
            return carry

        lax.fori_loop(0, width // wide, project_out, 0)
        pltpu.make_async_copy(out_v.at[sample], out_hbm.at[sample], local_sem.at[9 + sample]).start()

    drain(rx_v, stage_sem.at[0])
    drain(rz_v, stage_sem.at[2])
    drain(mod_v.at[pl.ds(0, nt * nx - 1)], stage_sem.at[4])
    drain(ckv_v.at[pl.ds(0, nsp - 1)], stage_sem.at[6])
    for copy in (to_after, to_before, on_after, on_before, over_before, over_after, over_across):
        copy.wait_send()

    @pl.when(sp < nsp - 1)
    def _():
        send_right.wait_send()

    @pl.when(sp > 0)
    def _():
        send_left.wait_send()

    for k in range(nt - 1):
        for sample in range(samples):
            att_copy(k, sample, lax.rem(tp + 1 + k, nt)).wait_send()
    for sample in range(samples):
        pltpu.make_async_copy(out_v.at[sample], out_hbm.at[sample], local_sem.at[9 + sample]).wait()


def shards(
    sizes, latent, context, condition, ctx_cond, norm_gain, w_shift, w_scale, w_gate, w_query, w_key, w_value, w_out,
    sink_logit, ctx_lift,
):
    nsp, nx, nt, nd = sizes
    nz = nsp // nx
    samples, tokens, width = latent.shape
    ctx_local = context.shape[1]
    ctx = ctx_local * nsp
    feats = condition.shape[1]
    cols = w_shift.shape[1]
    chunk = tokens // nt
    keys = ctx + tokens + 2 * WINDOW
    own_rows = w_out.shape[0]
    anywhere = pl.BlockSpec(memory_space=pl.ANY)
    vmem = pl.BlockSpec(memory_space=pltpu.VMEM)
    smem = pl.BlockSpec(memory_space=pltpu.SMEM)
    dma = pltpu.SemaphoreType.DMA
    return pl.pallas_call(
        functools.partial(layer, sizes),
        out_shape=jax.ShapeDtypeStruct((samples, chunk, width), bf16),
        in_specs=[anywhere, anywhere, vmem, vmem, vmem] + [anywhere] * 7 + [smem, smem],
        out_specs=anywhere,
        scratch_shapes=[
            pltpu.VMEM((samples, tokens, width), bf16),
            pltpu.VMEM((samples, ctx_local, width), bf16),
            pltpu.VMEM((3, feats, cols), bf16),
            pltpu.VMEM((width, 4 * HEAD), bf16),
            pltpu.VMEM((width, HEAD), bf16),
            pltpu.VMEM((width, HEAD), bf16),
            pltpu.VMEM((width, LANES), bf16),
            pltpu.VMEM((own_rows * nt, width), bf16),
            pltpu.VMEM((16, feats), f32),
            pltpu.VMEM((nx, 8, LANES), f32),
            pltpu.VMEM((nx - 1, 8, LANES), f32),
            pltpu.VMEM((8, LANES), f32),
            pltpu.VMEM((nz - 1, 8, LANES), f32),
            pltpu.VMEM((nt * nx, 8, LANES), f32),
            pltpu.VMEM((8, width), f32),
            pltpu.VMEM((samples, 8, width), f32),
            pltpu.VMEM((samples, 8, width), f32),
            pltpu.VMEM((samples, tokens, LANES), f32),
            pltpu.VMEM((tokens, LANES), f32),
            pltpu.VMEM((tokens, LANES), f32),
            pltpu.VMEM((samples, 4, tokens, LANES), bf16),
            pltpu.VMEM((samples, tokens + 2 * WINDOW, LANES), bf16),
            pltpu.VMEM((nsp, samples, ctx_local, LANES), bf16),
            pltpu.VMEM((samples, LANES, keys), bf16),
            pltpu.VMEM((samples, keys, 2 * LANES), bf16),
            pltpu.VMEM((samples, tokens, 2 * LANES), bf16),
            pltpu.VMEM((nt, samples, chunk, 2 * LANES), bf16),
            pltpu.VMEM((samples, chunk, width), bf16),
            dma((9 + samples,)),
            dma((8,)),
            dma((2,)),
            dma((2,)),
            dma((7,)),
            dma((7,)),
            dma((nt - 1, samples)),
            dma((nt - 1, samples)),
        ],
        compiler_params=pltpu.CompilerParams(
            collective_id=0, has_side_effects=True, vmem_limit_bytes=62 * 1024 * 1024
        ),
        name="layer",
    )(
        latent, context, condition, ctx_cond.reshape(1, feats), norm_gain.reshape(1, width), w_shift, w_scale, w_gate,
        w_query, w_key, w_value, w_out, sink_logit, ctx_lift,
    )


def solution(mesh):
    nsp, nt, nd = mesh.shape["sp"], mesh.shape["tp"], mesh.shape["dp"]
    sizes = (nsp, 4 if nsp > 4 else 2, nt, nd)
    return jax.shard_map(
        functools.partial(shards, sizes),
        mesh=mesh,
        in_specs=(
            P("dp", "sp", None),
            P("dp", "sp", None),
            P("dp", "sp"),
            P("sp"),
            P(),
            P("sp", "tp"),
            P("sp", "tp"),
            P("sp", "tp"),
            P(None, "tp"),
            P(None, "tp"),
            P(None, "tp"),
            P("tp", None),
            P("tp"),
            P("tp"),
        ),
        out_specs=P("dp", ("sp", "tp"), None),
        check_vma=False,
    )
```

```python
import functools
import math

import jax
import jax.numpy as jnp
from jax import lax
from jax.experimental import pallas as pl
from jax.experimental.pallas import tpu as pltpu
from jax.sharding import PartitionSpec as P

HEAD = 64
WINDOW = 128
GRID_COLS = 64
EPSILON = 1e-06
ROPE_BASE = 10000.0
NEGATIVE = -1e30
LOG2E = math.log2(math.e)
LANES = 128
MESH = pl.DeviceIdType.MESH
f32 = jnp.float32
bf16 = jnp.bfloat16


def lanes_of(rows):
    return lax.broadcasted_iota(jnp.int32, (rows, LANES), 1)


def drain(ref, sem):
    pltpu.make_async_copy(ref, ref, sem).wait()


def swapped(u, lane):
    return jnp.where(lane % 32 < 16, pltpu.roll(u, LANES - 16, 1), pltpu.roll(u, 16, 1))


class Scores:
    def __init__(self, refs, sample, row, left_off, right_off, score_ref, top_ref):
        self.kv, self.ckv, q_ref, self.limits = refs
        self.sample, self.row, self.offsets = sample, row, {0: left_off, 2 * WINDOW: right_off}
        self.score_ref, self.top_ref = score_ref, top_ref
        turned = q_ref[sample, pl.ds(row, WINDOW), :].astype(f32).T.astype(bf16)
        self.q = jnp.concatenate([turned[h * HEAD : (h + 1) * HEAD] for h in range(4)], axis=1)
        self.tops = {}

    def piece(self, kind, at, put, rows):
        ctx_local = self.ckv.shape[2]
        if kind == "far":
            keys = self.ckv[self.sample, at // ctx_local : (at + rows) // ctx_local].reshape(rows, LANES)
        else:
            keys = self.kv[self.sample, pl.ds(pl.multiple_of(self.row + at, WINDOW), rows), :]
        score = jnp.dot(keys[:, :HEAD], self.q, preferred_element_type=f32)
        if kind == "near" and at != WINDOW:
            key = lax.broadcasted_iota(jnp.int32, score.shape, 0)
            query = lax.broadcasted_iota(jnp.int32, score.shape, 1) % WINDOW
            inside = key >= query if at == 0 else key <= query
            score = jnp.where(inside, score, NEGATIVE) + self.offsets[at]
        self.score_ref[put : put + rows, :] = score
        top = jnp.max(score.reshape(rows // 8, 8, score.shape[1]), axis=0)
        self.tops[kind] = jnp.maximum(self.tops[kind], top) if kind in self.tops else top

    def done(self):
        far = jnp.max(self.tops["far"], axis=0, keepdims=True) + self.limits[0:1, :]
        near = jnp.max(self.tops["near"], axis=0, keepdims=True)
        self.top_ref[0:1, :] = jnp.maximum(jnp.maximum(far, near), self.limits[1:2, :])


class Weights:
    def __init__(self, vt, limits, att, ctx, sample, row, score_ref, top_ref):
        self.vt, self.att, self.ctx, self.sample, self.row, self.score_ref = vt, att, ctx, sample, row, score_ref
        self.top = top_ref[0:1, :]
        self.lowered = self.top - limits[0:1, :]
        self.sink = jnp.exp2(limits[1:2, :] - self.top)
        self.total = jnp.zeros((vt.shape[1], 4 * WINDOW), f32)

    def piece(self, kind, at, put, rows):
        top = self.lowered if kind == "far" else self.top
        weight = jnp.exp2(self.score_ref[put : put + rows, :] - top).astype(bf16)
        if kind == "far":
            values = self.vt[self.sample, :, at : at + rows]
        else:
            values = self.vt[self.sample, :, pl.ds(pl.multiple_of(self.ctx + self.row + at, WINDOW), rows)]
        self.total = self.total + jnp.dot(values, weight, preferred_element_type=f32)

    def done(self):
        out = self.total[16:] * (1.0 / (self.total[0:1] + self.sink))
        stacked = jnp.concatenate([out[:, h * WINDOW : (h + 1) * WINDOW] for h in range(4)], axis=0)
        self.att[self.sample, pl.ds(self.row, WINDOW), :] = stacked.T.astype(bf16)


def layer(
    sizes,
    x_hbm, context_hbm, condition, ctx_cond, gain, wsh_hbm, wsc_hbm, wga_hbm, wq_hbm, wk_hbm, wv_hbm, wo_hbm,
    sink_ref, lift_ref,
    out_v,
    x_v, context_v, wm_v, wq_v, wt_v, wkv_v, wo_v,
    active_v, part_v, rx_v, zsrc_v, rz_v, mod_v, modr_v, mul_v, add_v,
    inv_v, cos_v, sin_v, q_v, kv_v, ckv_v, vt_v, limits_v, s0_v, s1_v, t0_v, t1_v, att_v, by_v,
    local_sem, stage_sem, ctx_sem, halo_send, halo_recv, wo_send, wo_recv, att_send, att_recv,
):
    nsp, nx, nt, nd = sizes
    nz = nsp // nx
    samples, tokens, width = x_v.shape
    chunk = tokens // nt
    ctx_local = context_v.shape[1]
    ctx = ctx_local * nsp
    sp = lax.axis_index("sp")
    tp = lax.axis_index("tp")
    dp = lax.axis_index("dp")
    xi = lax.rem(sp, nx)
    zi = lax.div(sp, nx)

    def place(sp_to=None, tp_to=None, dp_to=None):
        return {
            "sp": sp if sp_to is None else sp_to,
            "tp": tp if tp_to is None else tp_to,
            "dp": dp if dp_to is None else dp_to,
        }

    def remote(src, dst, send, recv, device):
        return pltpu.make_async_remote_copy(
            src_ref=src, dst_ref=dst, send_sem=send, recv_sem=recv, device_id=device, device_id_type=MESH
        )

    def x_peer(offset):
        return zi * nx + lax.rem(xi + offset, nx)

    def z_peer(offset):
        return lax.rem(zi + offset, nz) * nx + xi

    own_rows = wo_hbm.shape[0]
    half = own_rows // nd
    loads = [
        pltpu.make_async_copy(wsh_hbm, wm_v.at[0], local_sem.at[0]),
        pltpu.make_async_copy(wsc_hbm, wm_v.at[1], local_sem.at[1]),
        pltpu.make_async_copy(wga_hbm, wm_v.at[2], local_sem.at[2]),
        pltpu.make_async_copy(
            wo_hbm, wo_v.at[pl.ds(pl.multiple_of(tp * own_rows, own_rows), own_rows), :], local_sem.at[3]
        ),
        pltpu.make_async_copy(context_hbm, context_v, local_sem.at[4]),
        pltpu.make_async_copy(x_hbm, x_v, local_sem.at[5]),
        pltpu.make_async_copy(wk_hbm, wt_v.at[pl.ds(0, HEAD), :], local_sem.at[6]),
        pltpu.make_async_copy(wv_hbm, wt_v.at[pl.ds(HEAD, HEAD), :], local_sem.at[7]),
        pltpu.make_async_copy(wq_hbm, wq_v, local_sem.at[8]),
    ]
    for load in loads:
        load.start()

    barrier = pltpu.get_barrier_semaphore()

    def greet(device):
        pl.semaphore_signal(barrier, inc=1, device_id=device, device_id_type=MESH)

    for offset in range(1, nx):
        greet(place(sp_to=x_peer(offset)))
    for offset in range(1, nz):
        greet(place(sp_to=z_peer(offset)))
    for offset in range(1, nt):
        greet(place(tp_to=lax.rem(tp + offset, nt)))
    for offset in range(1, nd):
        greet(place(dp_to=lax.rem(dp + offset, nd)))

    active_v[...] = jnp.zeros_like(active_v)
    active_v[0:2, :] = condition[...].astype(f32)
    active_v[2:3, :] = ctx_cond[...].astype(f32)
    raw = active_v[...]
    active = (raw / (1.0 + jnp.exp(-raw))).astype(bf16)
    for load in loads[:3]:
        load.wait()
    vecs = [jnp.dot(active, wm_v[k], preferred_element_type=f32) for k in range(3)]
    for c in range(nx):
        cols = slice(c * LANES, (c + 1) * LANES)
        part_v[c, 0:3, :] = vecs[0][0:3, cols]
        part_v[c, 3:6, :] = vecs[1][0:3, cols]
        part_v[c, 6:8, :] = vecs[2][0:2, cols]

    pl.semaphore_wait(barrier, (nx - 1) + (nz - 1) + (nt - 1) + (nd - 1))

    for offset in range(1, nx):
        to = lax.rem(xi + offset, nx)
        remote(part_v.at[to], rx_v.at[offset - 1], stage_sem.at[0], stage_sem.at[1], place(sp_to=x_peer(offset))).start()

    loads[3].wait()

    def wo_rows(owner, core, start, count):
        return wo_v.at[pl.ds(pl.multiple_of(owner * own_rows + core * half + start, count), count), :]

    after = lax.rem(tp + 1, nt)
    before = lax.rem(tp + nt - 1, nt)
    across = lax.rem(tp + 2, nt)
    other = lax.rem(dp + 1, nd)
    quarter = half // 2

    def wo_copy(k, ref, device):
        return remote(ref, ref, wo_send.at[k], wo_recv.at[k], device)

    wo_sends = [
        wo_copy(0, wo_rows(tp, dp, 0, quarter), place(tp_to=after)),
        wo_copy(1, wo_rows(tp, dp, 0, quarter), place(tp_to=before)),
        wo_copy(2, wo_rows(tp, dp, quarter, quarter), place(tp_to=after)),
        wo_copy(3, wo_rows(tp, dp, quarter, quarter), place(tp_to=before)),
        wo_copy(4, wo_rows(before, dp, 0, quarter), place(tp_to=after)),
        wo_copy(5, wo_rows(after, dp, quarter, quarter), place(tp_to=before)),
        wo_copy(6, wo_rows(before, dp, 0, half), place(dp_to=other)),
        wo_copy(7, wo_rows(after, dp, 0, half), place(dp_to=other)),
        wo_copy(8, wo_rows(across, dp, 0, half), place(dp_to=other)),
    ]
    wo_sends[0].start()
    wo_sends[1].start()

    block = min(256, chunk)
    blocks = tokens // block

    def statistics(step):
        sample, start = step // blocks, pl.multiple_of(step % blocks * block, block)
        total = jnp.zeros((block, LANES), f32)
        for c in range(width // LANES):
            piece = x_v[sample, pl.ds(start, block), c * LANES : (c + 1) * LANES].astype(f32)
            total = total + piece * piece
        mean = jnp.sum(total, axis=1, keepdims=True) / width
        inv_v[sample, pl.ds(start, block), :] = jnp.broadcast_to(lax.rsqrt(mean + EPSILON), (block, LANES))

    loads[6].wait()
    loads[7].wait()
    wkv_v[...] = wt_v[...].T
    loads[5].wait()

    def stats_loop(first, last):
        def run(step, carry):
            statistics(step)
            return carry

        lax.fori_loop(first, last, run, 0)

    all_blocks = samples * blocks
    stats_loop(0, all_blocks // 2)

    drain(rx_v, stage_sem.at[1])
    quarter_sum = part_v[xi]
    for k in range(nx - 1):
        quarter_sum = quarter_sum + rx_v[k]
    zsrc_v[...] = quarter_sum

    for offset in range(1, nz):
        remote(zsrc_v, rz_v.at[offset - 1], stage_sem.at[2], stage_sem.at[3], place(sp_to=z_peer(offset))).start()

    stats_loop(all_blocks // 2, all_blocks)
    lane1 = lanes_of(8)
    frequency = jnp.exp((lane1[0:1] % 16).astype(f32) * (-math.log(ROPE_BASE) / 16.0))
    grid_rows = tokens // GRID_COLS
    table_rows = max(grid_rows, 8)
    row_pos = (sp * grid_rows + lax.broadcasted_iota(jnp.int32, (table_rows, LANES), 0)).astype(f32)
    col_pos = lax.broadcasted_iota(jnp.int32, (GRID_COLS, LANES), 0).astype(f32)
    row_cos, row_sin = jnp.cos(row_pos * frequency), jnp.sin(row_pos * frequency)
    col_cos, col_sin = jnp.cos(col_pos * frequency), jnp.sin(col_pos * frequency)
    lane64 = lanes_of(GRID_COLS)
    by_row = lane64 % HEAD < 32
    minus = lane64 % 32 < 16
    for t in range(grid_rows):
        rows = slice(t * GRID_COLS, (t + 1) * GRID_COLS)
        cos_v[rows, :] = jnp.where(by_row, row_cos[t : t + 1, :], col_cos)
        sine = jnp.where(by_row, row_sin[t : t + 1, :], col_sin)
        sin_v[rows, :] = jnp.where(minus, -sine, sine)

    drain(rz_v, stage_sem.at[3])
    total = zsrc_v[...]
    for k in range(nz - 1):
        total = total + rz_v[k]
    here = tp * nx + xi
    mod_v[here] = total

    for dy in range(nt):
        for dx in range(nx):
            if dy or dx:
                remote(
                    mod_v.at[here], mod_v.at[here], stage_sem.at[4], stage_sem.at[5],
                    place(sp_to=x_peer(dx), tp_to=lax.rem(tp + dy, nt)),
                ).start()

    wo_sends[0].wait_recv()
    wo_sends[4].start()
    wo_sends[2].start()
    wo_sends[3].start()

    @pl.when(sp == 0)
    def _():
        kv_v[:, 0:WINDOW, :] = jnp.zeros((samples, WINDOW, LANES), bf16)

    @pl.when(sp == nsp - 1)
    def _():
        kv_v[:, WINDOW + tokens :, :] = jnp.zeros((samples, WINDOW, LANES), bf16)

    loads[4].wait()
    loads[8].wait()
    ctx_rows = samples * ctx_local
    ctx_wide = context_v[...].reshape(ctx_rows, width).astype(f32)
    ctx_inv = lax.rsqrt(jnp.mean(ctx_wide * ctx_wide, axis=1, keepdims=True) + EPSILON)
    ctx_unit = ctx_wide * ctx_inv

    drain(mod_v.at[pl.ds(0, nt * nx - 1)], stage_sem.at[5])
    for k in range(nt * nx):
        modr_v[:, k * LANES : (k + 1) * LANES] = mod_v[k]
    scaled = gain[...] * (1.0 + modr_v[3:6, :])
    for r in range(samples):
        mul_v[r, 0:1, :] = scaled[r : r + 1]
        add_v[r, 0:1, :] = modr_v[r : r + 1, :]

    ctx_hidden = (ctx_unit * scaled[2:3] + modr_v[2:3, :]).astype(bf16)
    ctx_pairs = jnp.dot(ctx_hidden, wkv_v[...], preferred_element_type=f32).astype(bf16)
    ckv_v[:, pl.ds(sp, 1)] = ctx_pairs.reshape(samples, 1, ctx_local, LANES)

    def ctx_rows_of(owner):
        return ckv_v.at[:, pl.ds(owner, 1)]

    def ctx_along_x(owner_z):
        rows = ctx_rows_of(owner_z * nx + xi)
        for offset in range(1, nx):
            remote(rows, rows, stage_sem.at[6], stage_sem.at[7], place(sp_to=x_peer(offset))).start()

    def ctx_along_z(offset):
        rows = ctx_rows_of(sp)
        return remote(rows, rows, ctx_sem.at[0, offset], ctx_sem.at[1, offset], place(sp_to=z_peer(offset)))

    for offset in range(1, nz):
        ctx_along_z(offset).start()
    ctx_along_x(zi)

    def pass_on(offsets):
        for offset in offsets:
            ctx_along_z(offset).wait_recv()
            ctx_along_x(lax.rem(zi + nz - offset, nz))

    far_z = [offset for offset in range(1, nz) if 2 < offset < nz - 2]
    near_z = [offset for offset in range(1, nz) if offset not in far_z]

    lane = lanes_of(block)
    low = lane < HEAD

    assert blocks == 4 and samples == 2
    steps = 4
    deep = width // steps
    factor = HEAD ** (-0.5) * LOG2E

    def block_of(step):
        late, turn = step // 4, step % 4
        index = (1 - late) * (turn % 2) * (blocks - 1) + late * (1 + turn % 2)
        return turn // 2, pl.multiple_of(index * block, block)

    def store_values(pairs_t, sample, start):
        vt_v[sample, 16:, pl.ds(start, pairs_t.shape[1])] = pairs_t[HEAD:].astype(bf16)

    def project(step):
        sample, start = block_of(step)
        inverse = inv_v[sample, pl.ds(start, block), :]
        q_acc = jnp.zeros((block, 2 * LANES), f32)
        kv_acc = jnp.zeros((block, LANES), f32)
        for k in range(steps):
            hidden = []
            for c in range(deep // LANES):
                cols = slice(k * deep + c * LANES, k * deep + (c + 1) * LANES)
                wide = x_v[sample, pl.ds(start, block), cols].astype(f32)
                hidden.append((wide * inverse * mul_v[sample, 0:1, cols] + add_v[sample, 0:1, cols]).astype(bf16))
            hidden = jnp.concatenate(hidden, axis=1)
            q_acc = q_acc + jnp.dot(hidden, wq_v[k * deep : (k + 1) * deep, :], preferred_element_type=f32)
            kv_acc = kv_acc + jnp.dot(hidden, wkv_v[k * deep : (k + 1) * deep, :], preferred_element_type=f32)
        cosine = cos_v[pl.ds(start, block), :]
        sine = sin_v[pl.ds(start, block), :]
        turned = jnp.where(low, kv_acc * cosine + swapped(kv_acc, lane) * sine, kv_acc)
        kv_v[sample, pl.ds(pl.multiple_of(WINDOW + start, WINDOW), block), :] = turned.astype(bf16)
        store_values(turned.T, sample, pl.multiple_of(ctx + WINDOW + start, WINDOW))
        for pair in range(2):
            u = q_acc[:, pair * LANES : (pair + 1) * LANES]
            turned = (u * cosine + swapped(u, lane) * sine) * factor
            q_v[sample, pl.ds(start, block), pair * LANES : (pair + 1) * LANES] = turned.astype(bf16)

    send_right = remote(
        kv_v.at[:, pl.ds(tokens, WINDOW), :], kv_v.at[:, pl.ds(0, WINDOW), :], halo_send.at[0], halo_recv.at[0],
        place(sp_to=lax.rem(sp + 1, nsp)),
    )
    send_left = remote(
        kv_v.at[:, pl.ds(WINDOW, WINDOW), :], kv_v.at[:, pl.ds(WINDOW + tokens, WINDOW), :], halo_send.at[1],
        halo_recv.at[1], place(sp_to=lax.rem(sp + nsp - 1, nsp)),
    )

    def project_group(group, carry):
        for member in range(4):
            project(4 * group + member)

        @pl.when((group == 0) & (sp < nsp - 1))
        def _():
            send_right.start()

        @pl.when((group == 0) & (sp > 0))
        def _():
            send_left.start()

        @pl.when(group == 0)
        def _():
            pass_on(near_z)

        @pl.when(group == 1)
        def _():
            pass_on(far_z)

        return carry

    lax.fori_loop(0, 2, project_group, 0)

    wo_sends[3].wait_recv()
    wo_sends[5].start()
    wo_sends[1].wait_recv()
    wo_sends[2].wait_recv()
    wo_sends[6].start()
    wo_sends[7].start()

    @pl.when(sp > 0)
    def _():
        send_right.wait_recv()

    @pl.when(sp < nsp - 1)
    def _():
        send_left.wait_recv()

    for sample in range(samples):
        store_values(kv_v[sample, :WINDOW].astype(f32).T, sample, ctx)
        store_values(kv_v[sample, WINDOW + tokens :].astype(f32).T, sample, ctx + WINDOW + tokens)
        vt_v[sample, :16, :] = jnp.ones((16, ctx + tokens + 2 * WINDOW), bf16)
    drain(ckv_v.at[:, pl.ds(0, nz * (nx - 1))], stage_sem.at[7])
    for sample in range(samples):
        store_values(ckv_v[sample].reshape(ctx, LANES).astype(f32).T, sample, 0)

    def att_copy(step_k, sample, dest):
        return remote(
            att_v.at[sample, pl.ds(pl.multiple_of(dest * chunk, chunk), chunk), :], by_v.at[tp, sample],
            att_send.at[step_k, sample], att_recv.at[step_k, sample], place(tp_to=dest),
        )

    limits_v[0:1, :] = jnp.concatenate([jnp.full((1, WINDOW), lift_ref[h] * LOG2E, f32) for h in range(4)], axis=1)
    limits_v[1:2, :] = jnp.concatenate([jnp.full((1, WINDOW), sink_ref[h] * LOG2E, f32) for h in range(4)], axis=1)
    subs = chunk // WINDOW
    deep_keys = min(256, ctx)
    pieces = [("far", c * deep_keys, c * deep_keys, deep_keys) for c in range(ctx // deep_keys)]
    pieces += [("near", c * WINDOW, ctx + c * WINDOW, WINDOW) for c in range(3)]
    buffers = ((s0_v, t0_v), (s1_v, t1_v))

    def rows_of(step, sub):
        k, sample = step // samples, step % samples
        dest = lax.rem(tp + 1 + k, nt)
        return sample, pl.multiple_of(dest * chunk + sub * WINDOW, WINDOW)

    def scores(step, buffer, sub):
        sample, row = rows_of(step, sub)
        left_off = jnp.where((sp == 0) & (row == 0), NEGATIVE, 0.0)
        right_off = jnp.where((sp == nsp - 1) & (row == tokens - WINDOW), NEGATIVE, 0.0)
        score_ref, top_ref = buffer
        return Scores((kv_v, ckv_v, q_v, limits_v), sample, row, left_off, right_off, score_ref.at[sub], top_ref.at[sub])

    def weights(step, buffer, sub):
        sample, row = rows_of(step, sub)
        score_ref, top_ref = buffer
        return Weights(vt_v, limits_v, att_v, ctx, sample, row, score_ref.at[sub], top_ref.at[sub])

    def both(now, later):
        for piece in pieces:
            for sub in range(subs):
                if now:
                    now[sub].piece(*piece)
                if later:
                    later[sub].piece(*piece)
        for sub in range(subs):
            if later:
                later[sub].done()
            if now:
                now[sub].done()

    both(None, [scores(0, buffers[0], sub) for sub in range(subs)])
    turns = nt * samples

    def chunk_step(step, carry):
        for parity in range(2):

            @pl.when(step % 2 == parity)
            def _():
                both(
                    [weights(step, buffers[parity], sub) for sub in range(subs)],
                    [scores(step + 1, buffers[1 - parity], sub) for sub in range(subs)],
                )

        k, sample = step // samples, step % samples

        @pl.when(k < nt - 1)
        def _():
            att_copy(k, sample, lax.rem(tp + 1 + k, nt)).start()

        @pl.when(step == 3)
        def _():
            wo_sends[4].wait_recv()
            wo_sends[5].wait_recv()
            wo_sends[8].start()

        return carry

    lax.fori_loop(0, turns - 1, chunk_step, 0)
    both([weights(turns - 1, buffers[(turns - 1) % 2], sub) for sub in range(subs)], None)
    by_v[tp] = att_v[:, pl.ds(pl.multiple_of(tp * chunk, chunk), chunk), :]

    for k in (6, 7, 8):
        wo_sends[k].wait_recv()
    for k in range(nt - 1):
        for sample in range(samples):
            att_copy(k, sample, lax.rem(tp + 1 + k, nt)).wait_recv()

    wide = min(1024, width)
    for sample in range(samples):

        def project_out(step, carry):
            cols = pl.ds(pl.multiple_of(step * wide, wide), wide)
            total = jnp.zeros((chunk, wide), f32)
            for t in range(nt):
                total = total + jnp.dot(
                    by_v[t, sample], wo_v[t * own_rows : (t + 1) * own_rows, cols], preferred_element_type=f32
                )
            out_v[sample, :, cols] = (total * modr_v[6 + sample : 7 + sample, cols]).astype(bf16)
            return carry

        lax.fori_loop(0, width // wide, project_out, 0)

    drain(rx_v, stage_sem.at[0])
    drain(rz_v, stage_sem.at[2])
    drain(mod_v.at[pl.ds(0, nt * nx - 1)], stage_sem.at[4])
    drain(ckv_v.at[:, pl.ds(0, nz * (nx - 1))], stage_sem.at[6])
    for offset in range(1, nz):
        ctx_along_z(offset).wait_send()
    for copy in wo_sends:
        copy.wait_send()

    @pl.when(sp < nsp - 1)
    def _():
        send_right.wait_send()

    @pl.when(sp > 0)
    def _():
        send_left.wait_send()

    for k in range(nt - 1):
        for sample in range(samples):
            att_copy(k, sample, lax.rem(tp + 1 + k, nt)).wait_send()


def shards(
    sizes, latent, context, condition, ctx_cond, norm_gain, w_shift, w_scale, w_gate, w_query, w_key, w_value, w_out,
    sink_logit, ctx_lift,
):
    nsp, nx, nt, nd = sizes
    nz = nsp // nx
    samples, tokens, width = latent.shape
    ctx_local = context.shape[1]
    ctx = ctx_local * nsp
    feats = condition.shape[1]
    cols = w_shift.shape[1]
    chunk = tokens // nt
    keys = ctx + tokens + 2 * WINDOW
    own_rows = w_out.shape[0]
    anywhere = pl.BlockSpec(memory_space=pltpu.HBM)
    vmem = pl.BlockSpec(memory_space=pltpu.VMEM)
    smem = pl.BlockSpec(memory_space=pltpu.SMEM)
    dma = pltpu.SemaphoreType.DMA
    return pl.pallas_call(
        functools.partial(layer, sizes),
        out_shape=pltpu.VMEM((samples, chunk, width), bf16),
        in_specs=[anywhere, anywhere, vmem, vmem, vmem] + [anywhere] * 7 + [smem, smem],
        out_specs=vmem,
        scratch_shapes=[
            pltpu.VMEM((samples, tokens, width), bf16),
            pltpu.VMEM((samples, ctx_local, width), bf16),
            pltpu.VMEM((3, feats, cols), bf16),
            pltpu.VMEM((width, 4 * HEAD), bf16),
            pltpu.VMEM((LANES, width), bf16),
            pltpu.VMEM((width, LANES), bf16),
            pltpu.VMEM((own_rows * nt, width), bf16),
            pltpu.VMEM((16, feats), f32),
            pltpu.VMEM((nx, 8, LANES), f32),
            pltpu.VMEM((nx - 1, 8, LANES), f32),
            pltpu.VMEM((8, LANES), f32),
            pltpu.VMEM((nz - 1, 8, LANES), f32),
            pltpu.VMEM((nt * nx, 8, LANES), f32),
            pltpu.VMEM((8, width), f32),
            pltpu.VMEM((samples, 8, width), f32),
            pltpu.VMEM((samples, 8, width), f32),
            pltpu.VMEM((samples, tokens, LANES), f32),
            pltpu.VMEM((tokens, LANES), f32),
            pltpu.VMEM((tokens, LANES), f32),
            pltpu.VMEM((samples, tokens, 4 * HEAD), bf16),
            pltpu.VMEM((samples, tokens + 2 * WINDOW, LANES), bf16),
            pltpu.VMEM((samples, nsp, ctx_local, LANES), bf16),
            pltpu.VMEM((samples, HEAD + 16, keys), bf16),
            pltpu.VMEM((8, 4 * WINDOW), f32),
            pltpu.VMEM((chunk // WINDOW, ctx + 3 * WINDOW, 4 * WINDOW), f32),
            pltpu.VMEM((chunk // WINDOW, ctx + 3 * WINDOW, 4 * WINDOW), f32),
            pltpu.VMEM((chunk // WINDOW, 8, 4 * WINDOW), f32),
            pltpu.VMEM((chunk // WINDOW, 8, 4 * WINDOW), f32),
            pltpu.VMEM((samples, tokens, 2 * LANES), bf16),
            pltpu.VMEM((nt, samples, chunk, 2 * LANES), bf16),
            dma((9,)),
            dma((8,)),
            dma((2, nz)),
            dma((2,)),
            dma((2,)),
            dma((9,)),
            dma((9,)),
            dma((nt - 1, samples)),
            dma((nt - 1, samples)),
        ],
        compiler_params=pltpu.CompilerParams(
            collective_id=0, has_side_effects=True, vmem_limit_bytes=61 * 1024 * 1024
        ),
        name="layer",
    )(
        latent, context, condition, ctx_cond.reshape(1, feats), norm_gain.reshape(1, width), w_shift, w_scale, w_gate,
        w_query, w_key.T, w_value.T, w_out, sink_logit, ctx_lift,
    )


def solution(mesh):
    nsp, nt, nd = mesh.shape["sp"], mesh.shape["tp"], mesh.shape["dp"]
    sizes = (nsp, 4 if nsp > 4 else 2, nt, nd)
    return jax.shard_map(
        functools.partial(shards, sizes),
        mesh=mesh,
        in_specs=(
            P("dp", "sp", None),
            P("dp", "sp", None),
            P("dp", "sp"),
            P("sp"),
            P(),
            P("sp", "tp"),
            P("sp", "tp"),
            P("sp", "tp"),
            P(None, "tp"),
            P(None, "tp"),
            P(None, "tp"),
            P("tp", None),
            P("tp"),
            P("tp"),
        ),
        out_specs=P("dp", ("sp", "tp"), None),
        check_vma=False,
    )
```

```python
import functools
import math

import jax
import jax.numpy as jnp
from jax import lax
from jax.experimental import pallas as pl
from jax.experimental.pallas import tpu as pltpu
from jax.sharding import PartitionSpec as P

HEAD = 64
WINDOW = 128
GRID_COLS = 64
EPSILON = 1e-06
ROPE_BASE = 10000.0
NEGATIVE = -1e30
LOG2E = math.log2(math.e)
LANES = 128
MESH = pl.DeviceIdType.MESH
f32 = jnp.float32
bf16 = jnp.bfloat16


def lanes_of(rows):
    return lax.broadcasted_iota(jnp.int32, (rows, LANES), 1)


def drain(ref, sem):
    pltpu.make_async_copy(ref, ref, sem).wait()


def swapped(u, lane):
    return jnp.where(lane % 32 < 16, pltpu.roll(u, LANES - 16, 1), pltpu.roll(u, 16, 1))


class Scores:
    def __init__(self, refs, sample, row, left_off, right_off, score_ref, top_ref):
        self.kv, self.ckv, q_ref, self.limits = refs
        self.sample, self.row, self.offsets = sample, row, {0: left_off, 2 * WINDOW: right_off}
        self.score_ref, self.top_ref = score_ref, top_ref
        turned = q_ref[sample, pl.ds(row, WINDOW), :].astype(f32).T.astype(bf16)
        self.q = jnp.concatenate([turned[h * HEAD : (h + 1) * HEAD] for h in range(4)], axis=1)
        self.tops = {}

    def piece(self, kind, at, put, rows):
        ctx_local = self.ckv.shape[2]
        if kind == "far":
            keys = self.ckv[self.sample, at // ctx_local : (at + rows) // ctx_local].reshape(rows, LANES)
        else:
            keys = self.kv[self.sample, pl.ds(pl.multiple_of(self.row + at, WINDOW), rows), :]
        score = jnp.dot(keys[:, :HEAD], self.q, preferred_element_type=f32)
        if kind == "near" and at != WINDOW:
            key = lax.broadcasted_iota(jnp.int32, score.shape, 0)
            query = lax.broadcasted_iota(jnp.int32, score.shape, 1) % WINDOW
            inside = key >= query if at == 0 else key <= query
            score = jnp.where(inside, score, NEGATIVE) + self.offsets[at]
        self.score_ref[put : put + rows, :] = score
        top = jnp.max(score.reshape(rows // 8, 8, score.shape[1]), axis=0)
        self.tops[kind] = jnp.maximum(self.tops[kind], top) if kind in self.tops else top

    def done(self):
        far = jnp.max(self.tops["far"], axis=0, keepdims=True) + self.limits[0:1, :]
        near = jnp.max(self.tops["near"], axis=0, keepdims=True)
        self.top_ref[0:1, :] = jnp.maximum(jnp.maximum(far, near), self.limits[1:2, :])


class Weights:
    def __init__(self, vt, limits, att, ctx, sample, row, score_ref, top_ref):
        self.vt, self.att, self.ctx, self.sample, self.row, self.score_ref = vt, att, ctx, sample, row, score_ref
        self.top = top_ref[0:1, :]
        self.lowered = self.top - limits[0:1, :]
        self.sink = jnp.exp2(limits[1:2, :] - self.top)
        self.total = jnp.zeros((vt.shape[1], 4 * WINDOW), f32)

    def piece(self, kind, at, put, rows):
        top = self.lowered if kind == "far" else self.top
        weight = jnp.exp2(self.score_ref[put : put + rows, :] - top).astype(bf16)
        if kind == "far":
            values = self.vt[self.sample, :, at : at + rows]
        else:
            values = self.vt[self.sample, :, pl.ds(pl.multiple_of(self.ctx + self.row + at, WINDOW), rows)]
        self.total = self.total + jnp.dot(values, weight, preferred_element_type=f32)

    def done(self):
        out = self.total[16:] * (1.0 / (self.total[0:1] + self.sink))
        stacked = jnp.concatenate([out[:, h * WINDOW : (h + 1) * WINDOW] for h in range(4)], axis=0)
        self.att[self.sample, pl.ds(self.row, WINDOW), :] = stacked.T.astype(bf16)


def layer(
    sizes,
    x_hbm, context_hbm, condition, ctx_cond, gain, wsh_hbm, wsc_hbm, wga_hbm, wq_hbm, wk_hbm, wv_hbm, wo_hbm,
    sink_ref, lift_ref,
    out_v,
    x_v, context_v, wm_v, wq_v, wt_v, wkv_v, wo_v,
    active_v, part_v, rx_v, zsrc_v, rz_v, mod_v, modr_v, mul_v, add_v,
    inv_v, cos_v, sin_v, q_v, kv_v, ckv_v, vt_v, limits_v, s0_v, s1_v, t0_v, t1_v, att_v, by_v,
    local_sem, stage_sem, ctx_sem, halo_send, halo_recv, wo_send, wo_recv, att_send, att_recv,
):
    nsp, nx, nt, nd = sizes
    nz = nsp // nx
    samples, tokens, width = x_v.shape
    chunk = tokens // nt
    ctx_local = context_v.shape[1]
    ctx = ctx_local * nsp
    sp = lax.axis_index("sp")
    tp = lax.axis_index("tp")
    dp = lax.axis_index("dp")
    xi = lax.rem(sp, nx)
    zi = lax.div(sp, nx)

    def place(sp_to=None, tp_to=None, dp_to=None):
        return {
            "sp": sp if sp_to is None else sp_to,
            "tp": tp if tp_to is None else tp_to,
            "dp": dp if dp_to is None else dp_to,
        }

    def remote(src, dst, send, recv, device):
        return pltpu.make_async_remote_copy(
            src_ref=src, dst_ref=dst, send_sem=send, recv_sem=recv, device_id=device, device_id_type=MESH
        )

    def x_peer(offset):
        return zi * nx + lax.rem(xi + offset, nx)

    def z_peer(offset):
        return lax.rem(zi + offset, nz) * nx + xi

    own_rows = wo_hbm.shape[0]
    half = own_rows // nd
    loads = [
        pltpu.make_async_copy(wsh_hbm, wm_v.at[0], local_sem.at[0]),
        pltpu.make_async_copy(wsc_hbm, wm_v.at[1], local_sem.at[1]),
        pltpu.make_async_copy(wga_hbm, wm_v.at[2], local_sem.at[2]),
        pltpu.make_async_copy(
            wo_hbm, wo_v.at[pl.ds(pl.multiple_of(tp * own_rows, own_rows), own_rows), :], local_sem.at[3]
        ),
        pltpu.make_async_copy(context_hbm, context_v, local_sem.at[4]),
        pltpu.make_async_copy(x_hbm, x_v, local_sem.at[5]),
        pltpu.make_async_copy(wk_hbm, wt_v.at[pl.ds(0, HEAD), :], local_sem.at[6]),
        pltpu.make_async_copy(wv_hbm, wt_v.at[pl.ds(HEAD, HEAD), :], local_sem.at[7]),
        pltpu.make_async_copy(wq_hbm, wq_v, local_sem.at[8]),
    ]
    for load in loads:
        load.start()

    barrier = pltpu.get_barrier_semaphore()

    def greet(device):
        pl.semaphore_signal(barrier, inc=1, device_id=device, device_id_type=MESH)

    for offset in range(1, nx):
        greet(place(sp_to=x_peer(offset)))
    for offset in range(1, nz):
        greet(place(sp_to=z_peer(offset)))
    for offset in range(1, nt):
        greet(place(tp_to=lax.rem(tp + offset, nt)))
    for offset in range(1, nd):
        greet(place(dp_to=lax.rem(dp + offset, nd)))

    active_v[...] = jnp.zeros_like(active_v)
    active_v[0:2, :] = condition[...].astype(f32)
    active_v[2:3, :] = ctx_cond[...].astype(f32)
    raw = active_v[...]
    active = (raw / (1.0 + jnp.exp(-raw))).astype(bf16)
    for load in loads[:3]:
        load.wait()
    vecs = [jnp.dot(active, wm_v[k], preferred_element_type=f32) for k in range(3)]
    for c in range(nx):
        cols = slice(c * LANES, (c + 1) * LANES)
        part_v[c, 0:3, :] = vecs[0][0:3, cols]
        part_v[c, 3:6, :] = vecs[1][0:3, cols]
        part_v[c, 6:8, :] = vecs[2][0:2, cols]

    pl.semaphore_wait(barrier, (nx - 1) + (nz - 1) + (nt - 1) + (nd - 1))

    for offset in range(1, nx):
        to = lax.rem(xi + offset, nx)
        remote(part_v.at[to], rx_v.at[offset - 1], stage_sem.at[0], stage_sem.at[1], place(sp_to=x_peer(offset))).start()

    loads[3].wait()

    def wo_rows(owner, core, start, count):
        return wo_v.at[pl.ds(pl.multiple_of(owner * own_rows + core * half + start, count), count), :]

    after = lax.rem(tp + 1, nt)
    before = lax.rem(tp + nt - 1, nt)
    across = lax.rem(tp + 2, nt)
    other = lax.rem(dp + 1, nd)
    quarter = half // 2

    def wo_copy(k, ref, device):
        return remote(ref, ref, wo_send.at[k], wo_recv.at[k], device)

    wo_sends = [
        wo_copy(0, wo_rows(tp, dp, 0, quarter), place(tp_to=after)),
        wo_copy(1, wo_rows(tp, dp, 0, quarter), place(tp_to=before)),
        wo_copy(2, wo_rows(tp, dp, quarter, quarter), place(tp_to=after)),
        wo_copy(3, wo_rows(tp, dp, quarter, quarter), place(tp_to=before)),
        wo_copy(4, wo_rows(before, dp, 0, quarter), place(tp_to=after)),
        wo_copy(5, wo_rows(after, dp, quarter, quarter), place(tp_to=before)),
        wo_copy(6, wo_rows(before, dp, 0, half), place(dp_to=other)),
        wo_copy(7, wo_rows(after, dp, 0, half), place(dp_to=other)),
        wo_copy(8, wo_rows(across, dp, 0, half), place(dp_to=other)),
    ]
    wo_sends[0].start()
    wo_sends[1].start()

    block = min(256, chunk)
    blocks = tokens // block

    def statistics(step):
        sample, start = step // blocks, pl.multiple_of(step % blocks * block, block)
        total = jnp.zeros((block, LANES), f32)
        for c in range(width // LANES):
            piece = x_v[sample, pl.ds(start, block), c * LANES : (c + 1) * LANES].astype(f32)
            total = total + piece * piece
        mean = jnp.sum(total, axis=1, keepdims=True) / width
        inv_v[sample, pl.ds(start, block), :] = jnp.broadcast_to(lax.rsqrt(mean + EPSILON), (block, LANES))

    loads[6].wait()
    loads[7].wait()
    wkv_v[...] = wt_v[...].T
    loads[5].wait()

    def stats_loop(first, last):
        def run(step, carry):
            statistics(step)
            return carry

        lax.fori_loop(first, last, run, 0)

    all_blocks = samples * blocks
    stats_loop(0, all_blocks // 2)

    drain(rx_v, stage_sem.at[1])
    quarter_sum = part_v[xi]
    for k in range(nx - 1):
        quarter_sum = quarter_sum + rx_v[k]
    zsrc_v[...] = quarter_sum

    for offset in range(1, nz):
        remote(zsrc_v, rz_v.at[offset - 1], stage_sem.at[2], stage_sem.at[3], place(sp_to=z_peer(offset))).start()

    stats_loop(all_blocks // 2, all_blocks)
    lane1 = lanes_of(8)
    frequency = jnp.exp((lane1[0:1] % 16).astype(f32) * (-math.log(ROPE_BASE) / 16.0))
    grid_rows = tokens // GRID_COLS
    table_rows = max(grid_rows, 8)
    row_pos = (sp * grid_rows + lax.broadcasted_iota(jnp.int32, (table_rows, LANES), 0)).astype(f32)
    col_pos = lax.broadcasted_iota(jnp.int32, (GRID_COLS, LANES), 0).astype(f32)
    row_cos, row_sin = jnp.cos(row_pos * frequency), jnp.sin(row_pos * frequency)
    col_cos, col_sin = jnp.cos(col_pos * frequency), jnp.sin(col_pos * frequency)
    lane64 = lanes_of(GRID_COLS)
    by_row = lane64 % HEAD < 32
    minus = lane64 % 32 < 16
    for t in range(grid_rows):
        rows = slice(t * GRID_COLS, (t + 1) * GRID_COLS)
        cos_v[rows, :] = jnp.where(by_row, row_cos[t : t + 1, :], col_cos)
        sine = jnp.where(by_row, row_sin[t : t + 1, :], col_sin)
        sin_v[rows, :] = jnp.where(minus, -sine, sine)

    drain(rz_v, stage_sem.at[3])
    total = zsrc_v[...]
    for k in range(nz - 1):
        total = total + rz_v[k]
    here = tp * nx + xi
    mod_v[here] = total

    for dy in range(nt):
        for dx in range(nx):
            if dy or dx:
                remote(
                    mod_v.at[here], mod_v.at[here], stage_sem.at[4], stage_sem.at[5],
                    place(sp_to=x_peer(dx), tp_to=lax.rem(tp + dy, nt)),
                ).start()

    wo_sends[0].wait_recv()
    wo_sends[4].start()
    wo_sends[2].start()
    wo_sends[3].start()

    @pl.when(sp == 0)
    def _():
        kv_v[:, 0:WINDOW, :] = jnp.zeros((samples, WINDOW, LANES), bf16)

    @pl.when(sp == nsp - 1)
    def _():
        kv_v[:, WINDOW + tokens :, :] = jnp.zeros((samples, WINDOW, LANES), bf16)

    loads[4].wait()
    loads[8].wait()
    ctx_rows = samples * ctx_local
    ctx_wide = context_v[...].reshape(ctx_rows, width).astype(f32)
    ctx_inv = lax.rsqrt(jnp.mean(ctx_wide * ctx_wide, axis=1, keepdims=True) + EPSILON)
    ctx_unit = ctx_wide * ctx_inv

    drain(mod_v.at[pl.ds(0, nt * nx - 1)], stage_sem.at[5])
    for k in range(nt * nx):
        modr_v[:, k * LANES : (k + 1) * LANES] = mod_v[k]
    scaled = gain[...] * (1.0 + modr_v[3:6, :])
    for r in range(samples):
        mul_v[r, 0:1, :] = scaled[r : r + 1]
        add_v[r, 0:1, :] = modr_v[r : r + 1, :]

    ctx_hidden = (ctx_unit * scaled[2:3] + modr_v[2:3, :]).astype(bf16)
    ctx_pairs = jnp.dot(ctx_hidden, wkv_v[...], preferred_element_type=f32).astype(bf16)
    ckv_v[:, pl.ds(sp, 1)] = ctx_pairs.reshape(samples, 1, ctx_local, LANES)

    def ctx_rows_of(owner):
        return ckv_v.at[:, pl.ds(owner, 1)]

    def ctx_along_x(owner_z):
        rows = ctx_rows_of(owner_z * nx + xi)
        for offset in range(1, nx):
            remote(rows, rows, stage_sem.at[6], stage_sem.at[7], place(sp_to=x_peer(offset))).start()

    def ctx_along_z(offset):
        rows = ctx_rows_of(sp)
        return remote(rows, rows, ctx_sem.at[0, offset], ctx_sem.at[1, offset], place(sp_to=z_peer(offset)))

    far_z = [offset for offset in range(1, nz) if 2 < offset < nz - 2]
    near_z = [offset for offset in range(1, nz) if offset not in far_z]
    for offset in near_z:
        ctx_along_z(offset).start()
    ctx_along_x(zi)
    own_pairs = ctx_rows_of(sp)
    for offset in far_z:
        ctx_along_z(offset).start()
        for dx in range(1, nx):
            to = lax.rem(zi + offset, nz) * nx + lax.rem(xi + dx, nx)
            remote(own_pairs, own_pairs, stage_sem.at[6], stage_sem.at[7], place(sp_to=to)).start()

    def pass_on(offsets):
        for offset in offsets:
            ctx_along_z(offset).wait_recv()
            ctx_along_x(lax.rem(zi + nz - offset, nz))

    lane = lanes_of(block)
    low = lane < HEAD

    assert blocks == 4 and samples == 2
    steps = 4
    deep = width // steps
    factor = HEAD ** (-0.5) * LOG2E

    def block_of(step):
        late, turn = step // 4, step % 4
        index = (1 - late) * (turn % 2) * (blocks - 1) + late * (1 + turn % 2)
        return turn // 2, pl.multiple_of(index * block, block)

    def store_values(pairs_t, sample, start):
        vt_v[sample, 16:, pl.ds(start, pairs_t.shape[1])] = pairs_t[HEAD:].astype(bf16)

    def project(step):
        sample, start = block_of(step)
        inverse = inv_v[sample, pl.ds(start, block), :]
        q_acc = jnp.zeros((block, 2 * LANES), f32)
        kv_acc = jnp.zeros((block, LANES), f32)
        for k in range(steps):
            hidden = []
            for c in range(deep // LANES):
                cols = slice(k * deep + c * LANES, k * deep + (c + 1) * LANES)
                wide = x_v[sample, pl.ds(start, block), cols].astype(f32)
                hidden.append((wide * inverse * mul_v[sample, 0:1, cols] + add_v[sample, 0:1, cols]).astype(bf16))
            hidden = jnp.concatenate(hidden, axis=1)
            q_acc = q_acc + jnp.dot(hidden, wq_v[k * deep : (k + 1) * deep, :], preferred_element_type=f32)
            kv_acc = kv_acc + jnp.dot(hidden, wkv_v[k * deep : (k + 1) * deep, :], preferred_element_type=f32)
        cosine = cos_v[pl.ds(start, block), :]
        sine = sin_v[pl.ds(start, block), :]
        turned = jnp.where(low, kv_acc * cosine + swapped(kv_acc, lane) * sine, kv_acc)
        kv_v[sample, pl.ds(pl.multiple_of(WINDOW + start, WINDOW), block), :] = turned.astype(bf16)
        store_values(turned.T, sample, pl.multiple_of(ctx + WINDOW + start, WINDOW))
        for pair in range(2):
            u = q_acc[:, pair * LANES : (pair + 1) * LANES]
            turned = (u * cosine + swapped(u, lane) * sine) * factor
            q_v[sample, pl.ds(start, block), pair * LANES : (pair + 1) * LANES] = turned.astype(bf16)

    send_right = remote(
        kv_v.at[:, pl.ds(tokens, WINDOW), :], kv_v.at[:, pl.ds(0, WINDOW), :], halo_send.at[0], halo_recv.at[0],
        place(sp_to=lax.rem(sp + 1, nsp)),
    )
    send_left = remote(
        kv_v.at[:, pl.ds(WINDOW, WINDOW), :], kv_v.at[:, pl.ds(WINDOW + tokens, WINDOW), :], halo_send.at[1],
        halo_recv.at[1], place(sp_to=lax.rem(sp + nsp - 1, nsp)),
    )

    def project_group(group, carry):
        for member in range(4):
            project(4 * group + member)

        @pl.when((group == 0) & (sp < nsp - 1))
        def _():
            send_right.start()

        @pl.when((group == 0) & (sp > 0))
        def _():
            send_left.start()

        @pl.when(group == 0)
        def _():
            pass_on(near_z)

        return carry

    lax.fori_loop(0, 2, project_group, 0)

    wo_sends[3].wait_recv()
    wo_sends[5].start()
    wo_sends[1].wait_recv()
    wo_sends[2].wait_recv()
    wo_sends[6].start()
    wo_sends[7].start()

    @pl.when(sp > 0)
    def _():
        send_right.wait_recv()

    @pl.when(sp < nsp - 1)
    def _():
        send_left.wait_recv()

    for sample in range(samples):
        store_values(kv_v[sample, :WINDOW].astype(f32).T, sample, ctx)
        store_values(kv_v[sample, WINDOW + tokens :].astype(f32).T, sample, ctx + WINDOW + tokens)
        vt_v[sample, :16, :] = jnp.ones((16, ctx + tokens + 2 * WINDOW), bf16)
    assert nt == 4

    def destination(k):
        late = k // 2
        return lax.rem(tp + (1 - late) * (2 - k) + late * (9 - 3 * k), nt)

    def att_copy(step_k, sample):
        dest = destination(step_k)
        return remote(
            att_v.at[sample, pl.ds(pl.multiple_of(dest * chunk, chunk), chunk), :], by_v.at[tp, sample],
            att_send.at[step_k, sample], att_recv.at[step_k, sample], place(tp_to=dest),
        )

    limits_v[0:1, :] = jnp.concatenate([jnp.full((1, WINDOW), lift_ref[h] * LOG2E, f32) for h in range(4)], axis=1)
    limits_v[1:2, :] = jnp.concatenate([jnp.full((1, WINDOW), sink_ref[h] * LOG2E, f32) for h in range(4)], axis=1)
    subs = chunk // WINDOW
    deep_keys = min(256, ctx)
    pieces = [("far", c * deep_keys, c * deep_keys, deep_keys) for c in range(ctx // deep_keys)]
    pieces += [("near", c * WINDOW, ctx + c * WINDOW, WINDOW) for c in range(3)]
    buffers = ((s0_v, t0_v), (s1_v, t1_v))

    def rows_of(step, sub):
        k, sample = step // samples, step % samples
        dest = destination(k)
        return sample, pl.multiple_of(dest * chunk + sub * WINDOW, WINDOW)

    def scores(step, buffer, sub):
        sample, row = rows_of(step, sub)
        left_off = jnp.where((sp == 0) & (row == 0), NEGATIVE, 0.0)
        right_off = jnp.where((sp == nsp - 1) & (row == tokens - WINDOW), NEGATIVE, 0.0)
        score_ref, top_ref = buffer
        return Scores((kv_v, ckv_v, q_v, limits_v), sample, row, left_off, right_off, score_ref.at[sub], top_ref.at[sub])

    def weights(step, buffer, sub):
        sample, row = rows_of(step, sub)
        score_ref, top_ref = buffer
        return Weights(vt_v, limits_v, att_v, ctx, sample, row, score_ref.at[sub], top_ref.at[sub])

    def both(now, later, only="all"):
        for piece in pieces:
            for sub in range(subs):
                if now and only == "all":
                    now[sub].piece(*piece)
                if later and only in ("all", piece[0]):
                    later[sub].piece(*piece)
        for sub in range(subs if only in ("all", None) else 0):
            if later:
                later[sub].done()
            if now:
                now[sub].done()

    start = [scores(0, buffers[0], sub) for sub in range(subs)]
    both(None, start, "near")

    for offset in far_z:
        ctx_along_z(offset).wait_recv()
    drain(ckv_v.at[:, pl.ds(0, nz * (nx - 1))], stage_sem.at[7])
    for sample in range(samples):
        store_values(ckv_v[sample].reshape(ctx, LANES).astype(f32).T, sample, 0)

    both(None, start, "far")
    both(None, start, None)
    turns = nt * samples

    def chunk_step(step, carry):
        for parity in range(2):

            @pl.when(step % 2 == parity)
            def _():
                both(
                    [weights(step, buffers[parity], sub) for sub in range(subs)],
                    [scores(step + 1, buffers[1 - parity], sub) for sub in range(subs)],
                )

        k, sample = step // samples, step % samples

        @pl.when(k < nt - 1)
        def _():
            att_copy(k, sample).start()

        @pl.when(step == 3)
        def _():
            wo_sends[4].wait_recv()
            wo_sends[5].wait_recv()
            wo_sends[8].start()

        return carry

    lax.fori_loop(0, turns - 1, chunk_step, 0)
    both([weights(turns - 1, buffers[(turns - 1) % 2], sub) for sub in range(subs)], None)
    by_v[tp] = att_v[:, pl.ds(pl.multiple_of(tp * chunk, chunk), chunk), :]

    for k in (6, 7, 8):
        wo_sends[k].wait_recv()
    wide = min(1024, width)
    for sample in range(samples):
        for k in range(nt - 1):
            att_copy(k, sample).wait_recv()

        def project_out(step, carry):
            cols = pl.ds(pl.multiple_of(step * wide, wide), wide)
            total = jnp.zeros((chunk, wide), f32)
            for t in range(nt):
                total = total + jnp.dot(
                    by_v[t, sample], wo_v[t * own_rows : (t + 1) * own_rows, cols], preferred_element_type=f32
                )
            out_v[sample, :, cols] = (total * modr_v[6 + sample : 7 + sample, cols]).astype(bf16)
            return carry

        lax.fori_loop(0, width // wide, project_out, 0)

    drain(rx_v, stage_sem.at[0])
    drain(rz_v, stage_sem.at[2])
    drain(mod_v.at[pl.ds(0, nt * nx - 1)], stage_sem.at[4])
    drain(ckv_v.at[:, pl.ds(0, nz * (nx - 1))], stage_sem.at[6])
    for offset in range(1, nz):
        ctx_along_z(offset).wait_send()
    for copy in wo_sends:
        copy.wait_send()

    @pl.when(sp < nsp - 1)
    def _():
        send_right.wait_send()

    @pl.when(sp > 0)
    def _():
        send_left.wait_send()

    for k in range(nt - 1):
        for sample in range(samples):
            att_copy(k, sample).wait_send()


def shards(
    sizes, latent, context, condition, ctx_cond, norm_gain, w_shift, w_scale, w_gate, w_query, w_key, w_value, w_out,
    sink_logit, ctx_lift,
):
    nsp, nx, nt, nd = sizes
    nz = nsp // nx
    samples, tokens, width = latent.shape
    ctx_local = context.shape[1]
    ctx = ctx_local * nsp
    feats = condition.shape[1]
    cols = w_shift.shape[1]
    chunk = tokens // nt
    keys = ctx + tokens + 2 * WINDOW
    own_rows = w_out.shape[0]
    anywhere = pl.BlockSpec(memory_space=pltpu.HBM)
    vmem = pl.BlockSpec(memory_space=pltpu.VMEM)
    smem = pl.BlockSpec(memory_space=pltpu.SMEM)
    dma = pltpu.SemaphoreType.DMA
    return pl.pallas_call(
        functools.partial(layer, sizes),
        out_shape=pltpu.VMEM((samples, chunk, width), bf16),
        in_specs=[anywhere, anywhere, vmem, vmem, vmem] + [anywhere] * 7 + [smem, smem],
        out_specs=vmem,
        scratch_shapes=[
            pltpu.VMEM((samples, tokens, width), bf16),
            pltpu.VMEM((samples, ctx_local, width), bf16),
            pltpu.VMEM((3, feats, cols), bf16),
            pltpu.VMEM((width, 4 * HEAD), bf16),
            pltpu.VMEM((LANES, width), bf16),
            pltpu.VMEM((width, LANES), bf16),
            pltpu.VMEM((own_rows * nt, width), bf16),
            pltpu.VMEM((16, feats), f32),
            pltpu.VMEM((nx, 8, LANES), f32),
            pltpu.VMEM((nx - 1, 8, LANES), f32),
            pltpu.VMEM((8, LANES), f32),
            pltpu.VMEM((nz - 1, 8, LANES), f32),
            pltpu.VMEM((nt * nx, 8, LANES), f32),
            pltpu.VMEM((8, width), f32),
            pltpu.VMEM((samples, 8, width), f32),
            pltpu.VMEM((samples, 8, width), f32),
            pltpu.VMEM((samples, tokens, LANES), f32),
            pltpu.VMEM((tokens, LANES), f32),
            pltpu.VMEM((tokens, LANES), f32),
            pltpu.VMEM((samples, tokens, 4 * HEAD), bf16),
            pltpu.VMEM((samples, tokens + 2 * WINDOW, LANES), bf16),
            pltpu.VMEM((samples, nsp, ctx_local, LANES), bf16),
            pltpu.VMEM((samples, HEAD + 16, keys), bf16),
            pltpu.VMEM((8, 4 * WINDOW), f32),
            pltpu.VMEM((chunk // WINDOW, ctx + 3 * WINDOW, 4 * WINDOW), f32),
            pltpu.VMEM((chunk // WINDOW, ctx + 3 * WINDOW, 4 * WINDOW), f32),
            pltpu.VMEM((chunk // WINDOW, 8, 4 * WINDOW), f32),
            pltpu.VMEM((chunk // WINDOW, 8, 4 * WINDOW), f32),
            pltpu.VMEM((samples, tokens, 2 * LANES), bf16),
            pltpu.VMEM((nt, samples, chunk, 2 * LANES), bf16),
            dma((9,)),
            dma((8,)),
            dma((2, nz)),
            dma((2,)),
            dma((2,)),
            dma((9,)),
            dma((9,)),
            dma((nt - 1, samples)),
            dma((nt - 1, samples)),
        ],
        compiler_params=pltpu.CompilerParams(
            collective_id=0, has_side_effects=True, vmem_limit_bytes=61 * 1024 * 1024
        ),
        name="layer",
    )(
        latent, context, condition, ctx_cond.reshape(1, feats), norm_gain.reshape(1, width), w_shift, w_scale, w_gate,
        w_query, w_key.T, w_value.T, w_out, sink_logit, ctx_lift,
    )


def solution(mesh):
    nsp, nt, nd = mesh.shape["sp"], mesh.shape["tp"], mesh.shape["dp"]
    sizes = (nsp, 4 if nsp > 4 else 2, nt, nd)
    return jax.shard_map(
        functools.partial(shards, sizes),
        mesh=mesh,
        in_specs=(
            P("dp", "sp", None),
            P("dp", "sp", None),
            P("dp", "sp"),
            P("sp"),
            P(),
            P("sp", "tp"),
            P("sp", "tp"),
            P("sp", "tp"),
            P(None, "tp"),
            P(None, "tp"),
            P(None, "tp"),
            P("tp", None),
            P("tp"),
            P("tp"),
        ),
        out_specs=P("dp", ("sp", "tp"), None),
        check_vma=False,
    )
```

```python
import functools
import math

import jax
import jax.numpy as jnp
from jax import lax
from jax.experimental import pallas as pl
from jax.experimental.pallas import tpu as pltpu
from jax.sharding import PartitionSpec as P

HEAD = 64
WINDOW = 128
GRID_COLS = 64
EPSILON = 1e-06
ROPE_BASE = 10000.0
NEGATIVE = -1e30
LOG2E = math.log2(math.e)
LANES = 128
MESH = pl.DeviceIdType.MESH
f32 = jnp.float32
bf16 = jnp.bfloat16


def lanes_of(rows):
    return lax.broadcasted_iota(jnp.int32, (rows, LANES), 1)


def drain(ref, sem):
    pltpu.make_async_copy(ref, ref, sem).wait()


def swapped(u, lane):
    return jnp.where(lane % 32 < 16, pltpu.roll(u, LANES - 16, 1), pltpu.roll(u, 16, 1))


class Scores:
    def __init__(self, refs, sample, row, left_off, right_off, score_ref, top_ref):
        self.kv, self.ckv, q_ref, self.limits = refs
        self.sample, self.row, self.offsets = sample, row, {0: left_off, 2 * WINDOW: right_off}
        self.score_ref, self.top_ref = score_ref, top_ref
        turned = q_ref[sample, pl.ds(row, WINDOW), :].astype(f32).T.astype(bf16)
        self.q = jnp.concatenate([turned[h * HEAD : (h + 1) * HEAD] for h in range(4)], axis=1)
        self.tops = {}

    def piece(self, kind, at, put, rows):
        ctx_local = self.ckv.shape[2]
        if kind == "far":
            keys = self.ckv[self.sample, at // ctx_local : (at + rows) // ctx_local].reshape(rows, LANES)
        else:
            keys = self.kv[self.sample, pl.ds(pl.multiple_of(self.row + at, WINDOW), rows), :]
        score = jnp.dot(keys[:, :HEAD], self.q, preferred_element_type=f32)
        if kind == "near" and at != WINDOW:
            key = lax.broadcasted_iota(jnp.int32, score.shape, 0)
            query = lax.broadcasted_iota(jnp.int32, score.shape, 1) % WINDOW
            inside = key >= query if at == 0 else key <= query
            score = jnp.where(inside, score, NEGATIVE) + self.offsets[at]
        self.score_ref[put : put + rows, :] = score
        top = jnp.max(score.reshape(rows // 8, 8, score.shape[1]), axis=0)
        self.tops[kind] = jnp.maximum(self.tops[kind], top) if kind in self.tops else top

    def done(self):
        far = jnp.max(self.tops["far"], axis=0, keepdims=True) + self.limits[0:1, :]
        near = jnp.max(self.tops["near"], axis=0, keepdims=True)
        self.top_ref[0:1, :] = jnp.maximum(jnp.maximum(far, near), self.limits[1:2, :])


class Weights:
    def __init__(self, vt, limits, att, ctx, sample, row, score_ref, top_ref):
        self.vt, self.att, self.ctx, self.sample, self.row, self.score_ref = vt, att, ctx, sample, row, score_ref
        self.top = top_ref[0:1, :]
        self.lowered = self.top - limits[0:1, :]
        self.sink = jnp.exp2(limits[1:2, :] - self.top)
        self.total = jnp.zeros((vt.shape[1], 4 * WINDOW), f32)

    def piece(self, kind, at, put, rows):
        top = self.lowered if kind == "far" else self.top
        weight = jnp.exp2(self.score_ref[put : put + rows, :] - top).astype(bf16)
        if kind == "far":
            values = self.vt[self.sample, :, at : at + rows]
        else:
            values = self.vt[self.sample, :, pl.ds(pl.multiple_of(self.ctx + self.row + at, WINDOW), rows)]
        self.total = self.total + jnp.dot(values, weight, preferred_element_type=f32)

    def done(self):
        out = self.total[16:] * (1.0 / (self.total[0:1] + self.sink))
        stacked = jnp.concatenate([out[:, h * WINDOW : (h + 1) * WINDOW] for h in range(4)], axis=0)
        self.att[self.sample, pl.ds(self.row, WINDOW), :] = stacked.T.astype(bf16)


def layer(
    sizes,
    x_hbm, context_hbm, condition_hbm, ctx_cond_hbm, gain_hbm, wsh_hbm, wsc_hbm, wga_hbm, wq_hbm, wk_hbm, wv_hbm, wo_hbm,
    sink_hbm, lift_hbm,
    out_v,
    condition, ctx_cond, gain, sink_ref, lift_ref, x_v, context_v, wm_v, wq_v, wt_v, wkv_v, wo_v,
    active_v, part_v, rx_v, zsrc_v, rz_v, mod_v, modr_v, mul_v, add_v,
    inv_v, cos_v, sin_v, q_v, kv_v, ckv_v, vt_v, limits_v, s0_v, s1_v, t0_v, t1_v, att_v, by_v,
    local_sem, stage_sem, ctx_sem, halo_send, halo_recv, wo_send, wo_recv, att_send, att_recv,
):
    nsp, nx, nt, nd = sizes
    nz = nsp // nx
    samples, tokens, width = x_v.shape
    chunk = tokens // nt
    ctx_local = context_v.shape[1]
    ctx = ctx_local * nsp
    sp = lax.axis_index("sp")
    tp = lax.axis_index("tp")
    dp = lax.axis_index("dp")
    xi = lax.rem(sp, nx)
    zi = lax.div(sp, nx)

    def place(sp_to=None, tp_to=None, dp_to=None):
        return {
            "sp": sp if sp_to is None else sp_to,
            "tp": tp if tp_to is None else tp_to,
            "dp": dp if dp_to is None else dp_to,
        }

    def remote(src, dst, send, recv, device):
        return pltpu.make_async_remote_copy(
            src_ref=src, dst_ref=dst, send_sem=send, recv_sem=recv, device_id=device, device_id_type=MESH
        )

    def x_peer(offset):
        return zi * nx + lax.rem(xi + offset, nx)

    def z_peer(offset):
        return lax.rem(zi + offset, nz) * nx + xi

    own_rows = wo_hbm.shape[0]
    half = own_rows // nd
    loads = [
        pltpu.make_async_copy(wsh_hbm, wm_v.at[0], local_sem.at[0]),
        pltpu.make_async_copy(wsc_hbm, wm_v.at[1], local_sem.at[1]),
        pltpu.make_async_copy(wga_hbm, wm_v.at[2], local_sem.at[2]),
        pltpu.make_async_copy(
            wo_hbm, wo_v.at[pl.ds(pl.multiple_of(tp * own_rows, own_rows), own_rows), :], local_sem.at[3]
        ),
        pltpu.make_async_copy(context_hbm, context_v, local_sem.at[4]),
        pltpu.make_async_copy(x_hbm, x_v, local_sem.at[5]),
        pltpu.make_async_copy(wk_hbm, wt_v.at[pl.ds(0, HEAD), :], local_sem.at[6]),
        pltpu.make_async_copy(wv_hbm, wt_v.at[pl.ds(HEAD, HEAD), :], local_sem.at[7]),
        pltpu.make_async_copy(wq_hbm, wq_v, local_sem.at[8]),
    ]
    small = [
        pltpu.make_async_copy(condition_hbm, condition, local_sem.at[9]),
        pltpu.make_async_copy(ctx_cond_hbm, ctx_cond, local_sem.at[10]),
        pltpu.make_async_copy(gain_hbm, gain, local_sem.at[11]),
        pltpu.make_async_copy(sink_hbm, sink_ref, local_sem.at[12]),
        pltpu.make_async_copy(lift_hbm, lift_ref, local_sem.at[13]),
    ]
    for load in small[:2] + loads + small[2:]:
        load.start()

    barrier = pltpu.get_barrier_semaphore()

    def greet(device):
        pl.semaphore_signal(barrier, inc=1, device_id=device, device_id_type=MESH)

    for offset in range(1, nx):
        greet(place(sp_to=x_peer(offset)))
    for offset in range(1, nz):
        greet(place(sp_to=z_peer(offset)))
    for offset in range(1, nt):
        greet(place(tp_to=lax.rem(tp + offset, nt)))
    for offset in range(1, nd):
        greet(place(dp_to=lax.rem(dp + offset, nd)))

    active_v[...] = jnp.zeros_like(active_v)
    for load in small[:2]:
        load.wait()
    active_v[0:2, :] = condition[...].astype(f32)
    active_v[2:3, :] = ctx_cond[...].astype(f32)
    raw = active_v[...]
    active = (raw / (1.0 + jnp.exp(-raw))).astype(bf16)
    for load in loads[:3]:
        load.wait()
    vecs = [jnp.dot(active, wm_v[k], preferred_element_type=f32) for k in range(3)]
    for c in range(nx):
        cols = slice(c * LANES, (c + 1) * LANES)
        part_v[c, 0:3, :] = vecs[0][0:3, cols]
        part_v[c, 3:6, :] = vecs[1][0:3, cols]
        part_v[c, 6:8, :] = vecs[2][0:2, cols]

    pl.semaphore_wait(barrier, (nx - 1) + (nz - 1) + (nt - 1) + (nd - 1))

    for offset in range(1, nx):
        to = lax.rem(xi + offset, nx)
        remote(part_v.at[to], rx_v.at[offset - 1], stage_sem.at[0], stage_sem.at[1], place(sp_to=x_peer(offset))).start()

    loads[3].wait()

    def wo_rows(owner, core, start, count):
        return wo_v.at[pl.ds(pl.multiple_of(owner * own_rows + core * half + start, count), count), :]

    after = lax.rem(tp + 1, nt)
    before = lax.rem(tp + nt - 1, nt)
    across = lax.rem(tp + 2, nt)
    other = lax.rem(dp + 1, nd)
    quarter = half // 2

    def wo_copy(k, ref, device):
        return remote(ref, ref, wo_send.at[k], wo_recv.at[k], device)

    wo_sends = [
        wo_copy(0, wo_rows(tp, dp, 0, quarter), place(tp_to=after)),
        wo_copy(1, wo_rows(tp, dp, 0, quarter), place(tp_to=before)),
        wo_copy(2, wo_rows(tp, dp, quarter, quarter), place(tp_to=after)),
        wo_copy(3, wo_rows(tp, dp, quarter, quarter), place(tp_to=before)),
        wo_copy(4, wo_rows(before, dp, 0, quarter), place(tp_to=after)),
        wo_copy(5, wo_rows(after, dp, quarter, quarter), place(tp_to=before)),
        wo_copy(6, wo_rows(before, dp, 0, half), place(dp_to=other)),
        wo_copy(7, wo_rows(after, dp, 0, half), place(dp_to=other)),
        wo_copy(8, wo_rows(across, dp, 0, half), place(dp_to=other)),
    ]
    wo_sends[0].start()
    wo_sends[1].start()

    block = min(256, chunk)
    blocks = tokens // block

    def statistics(step):
        sample, start = step // blocks, pl.multiple_of(step % blocks * block, block)
        total = jnp.zeros((block, LANES), f32)
        for c in range(width // LANES):
            piece = x_v[sample, pl.ds(start, block), c * LANES : (c + 1) * LANES].astype(f32)
            total = total + piece * piece
        mean = jnp.sum(total, axis=1, keepdims=True) / width
        inv_v[sample, pl.ds(start, block), :] = jnp.broadcast_to(lax.rsqrt(mean + EPSILON), (block, LANES))

    loads[6].wait()
    loads[7].wait()
    wkv_v[...] = wt_v[...].T
    loads[5].wait()

    def stats_loop(first, last):
        def run(step, carry):
            statistics(step)
            return carry

        lax.fori_loop(first, last, run, 0)

    all_blocks = samples * blocks
    stats_loop(0, all_blocks // 2)

    drain(rx_v, stage_sem.at[1])
    quarter_sum = part_v[xi]
    for k in range(nx - 1):
        quarter_sum = quarter_sum + rx_v[k]
    zsrc_v[...] = quarter_sum

    for offset in range(1, nz):
        remote(zsrc_v, rz_v.at[offset - 1], stage_sem.at[2], stage_sem.at[3], place(sp_to=z_peer(offset))).start()

    stats_loop(all_blocks // 2, all_blocks)
    lane1 = lanes_of(8)
    frequency = jnp.exp((lane1[0:1] % 16).astype(f32) * (-math.log(ROPE_BASE) / 16.0))
    grid_rows = tokens // GRID_COLS
    table_rows = max(grid_rows, 8)
    row_pos = (sp * grid_rows + lax.broadcasted_iota(jnp.int32, (table_rows, LANES), 0)).astype(f32)
    col_pos = lax.broadcasted_iota(jnp.int32, (GRID_COLS, LANES), 0).astype(f32)
    row_cos, row_sin = jnp.cos(row_pos * frequency), jnp.sin(row_pos * frequency)
    col_cos, col_sin = jnp.cos(col_pos * frequency), jnp.sin(col_pos * frequency)
    lane64 = lanes_of(GRID_COLS)
    by_row = lane64 % HEAD < 32
    minus = lane64 % 32 < 16
    for t in range(grid_rows):
        rows = slice(t * GRID_COLS, (t + 1) * GRID_COLS)
        cos_v[rows, :] = jnp.where(by_row, row_cos[t : t + 1, :], col_cos)
        sine = jnp.where(by_row, row_sin[t : t + 1, :], col_sin)
        sin_v[rows, :] = jnp.where(minus, -sine, sine)

    drain(rz_v, stage_sem.at[3])
    total = zsrc_v[...]
    for k in range(nz - 1):
        total = total + rz_v[k]
    here = tp * nx + xi
    mod_v[here] = total

    for dy in range(nt):
        for dx in range(nx):
            if dy or dx:
                remote(
                    mod_v.at[here], mod_v.at[here], stage_sem.at[4], stage_sem.at[5],
                    place(sp_to=x_peer(dx), tp_to=lax.rem(tp + dy, nt)),
                ).start()

    wo_sends[0].wait_recv()
    wo_sends[4].start()
    wo_sends[2].start()
    wo_sends[3].start()

    @pl.when(sp == 0)
    def _():
        kv_v[:, 0:WINDOW, :] = jnp.zeros((samples, WINDOW, LANES), bf16)

    @pl.when(sp == nsp - 1)
    def _():
        kv_v[:, WINDOW + tokens :, :] = jnp.zeros((samples, WINDOW, LANES), bf16)

    loads[4].wait()
    loads[8].wait()
    ctx_rows = samples * ctx_local
    ctx_wide = context_v[...].reshape(ctx_rows, width).astype(f32)
    ctx_inv = lax.rsqrt(jnp.mean(ctx_wide * ctx_wide, axis=1, keepdims=True) + EPSILON)
    ctx_unit = ctx_wide * ctx_inv

    drain(mod_v.at[pl.ds(0, nt * nx - 1)], stage_sem.at[5])
    for k in range(nt * nx):
        modr_v[:, k * LANES : (k + 1) * LANES] = mod_v[k]
    small[2].wait()
    scaled = gain[...] * (1.0 + modr_v[3:6, :])
    for r in range(samples):
        mul_v[r, 0:1, :] = scaled[r : r + 1]
        add_v[r, 0:1, :] = modr_v[r : r + 1, :]

    ctx_hidden = (ctx_unit * scaled[2:3] + modr_v[2:3, :]).astype(bf16)
    ctx_pairs = jnp.dot(ctx_hidden, wkv_v[...], preferred_element_type=f32).astype(bf16)
    ckv_v[:, pl.ds(sp, 1)] = ctx_pairs.reshape(samples, 1, ctx_local, LANES)

    def ctx_rows_of(owner):
        return ckv_v.at[:, pl.ds(owner, 1)]

    def ctx_along_x(owner_z):
        rows = ctx_rows_of(owner_z * nx + xi)
        for offset in range(1, nx):
            remote(rows, rows, stage_sem.at[6], stage_sem.at[7], place(sp_to=x_peer(offset))).start()

    def ctx_along_z(offset):
        rows = ctx_rows_of(sp)
        return remote(rows, rows, ctx_sem.at[0, offset], ctx_sem.at[1, offset], place(sp_to=z_peer(offset)))

    far_z = [offset for offset in range(1, nz) if 2 < offset < nz - 2]
    near_z = [offset for offset in range(1, nz) if offset not in far_z]
    for offset in near_z:
        ctx_along_z(offset).start()
    ctx_along_x(zi)
    own_pairs = ctx_rows_of(sp)
    for offset in far_z:
        ctx_along_z(offset).start()
        for dx in range(1, nx):
            to = lax.rem(zi + offset, nz) * nx + lax.rem(xi + dx, nx)
            remote(own_pairs, own_pairs, stage_sem.at[6], stage_sem.at[7], place(sp_to=to)).start()

    def pass_on(offsets):
        for offset in offsets:
            ctx_along_z(offset).wait_recv()
            ctx_along_x(lax.rem(zi + nz - offset, nz))

    lane = lanes_of(block)
    low = lane < HEAD

    assert blocks == 4 and samples == 2
    steps = 4
    deep = width // steps
    factor = HEAD ** (-0.5) * LOG2E

    def block_of(step):
        late, turn = step // 4, step % 4
        index = (1 - late) * (turn % 2) * (blocks - 1) + late * (1 + turn % 2)
        return turn // 2, pl.multiple_of(index * block, block)

    def store_values(pairs_t, sample, start):
        vt_v[sample, 16:, pl.ds(start, pairs_t.shape[1])] = pairs_t[HEAD:].astype(bf16)

    def project(step):
        sample, start = block_of(step)
        inverse = inv_v[sample, pl.ds(start, block), :]
        q_acc = jnp.zeros((block, 2 * LANES), f32)
        kv_acc = jnp.zeros((block, LANES), f32)
        for k in range(steps):
            hidden = []
            for c in range(deep // LANES):
                cols = slice(k * deep + c * LANES, k * deep + (c + 1) * LANES)
                wide = x_v[sample, pl.ds(start, block), cols].astype(f32)
                hidden.append((wide * inverse * mul_v[sample, 0:1, cols] + add_v[sample, 0:1, cols]).astype(bf16))
            hidden = jnp.concatenate(hidden, axis=1)
            q_acc = q_acc + jnp.dot(hidden, wq_v[k * deep : (k + 1) * deep, :], preferred_element_type=f32)
            kv_acc = kv_acc + jnp.dot(hidden, wkv_v[k * deep : (k + 1) * deep, :], preferred_element_type=f32)
        cosine = cos_v[pl.ds(start, block), :]
        sine = sin_v[pl.ds(start, block), :]
        turned = jnp.where(low, kv_acc * cosine + swapped(kv_acc, lane) * sine, kv_acc)
        kv_v[sample, pl.ds(pl.multiple_of(WINDOW + start, WINDOW), block), :] = turned.astype(bf16)
        store_values(turned.T, sample, pl.multiple_of(ctx + WINDOW + start, WINDOW))
        for pair in range(2):
            u = q_acc[:, pair * LANES : (pair + 1) * LANES]
            turned = (u * cosine + swapped(u, lane) * sine) * factor
            q_v[sample, pl.ds(start, block), pair * LANES : (pair + 1) * LANES] = turned.astype(bf16)

    send_right = remote(
        kv_v.at[:, pl.ds(tokens, WINDOW), :], kv_v.at[:, pl.ds(0, WINDOW), :], halo_send.at[0], halo_recv.at[0],
        place(sp_to=lax.rem(sp + 1, nsp)),
    )
    send_left = remote(
        kv_v.at[:, pl.ds(WINDOW, WINDOW), :], kv_v.at[:, pl.ds(WINDOW + tokens, WINDOW), :], halo_send.at[1],
        halo_recv.at[1], place(sp_to=lax.rem(sp + nsp - 1, nsp)),
    )

    def project_group(group, carry):
        for member in range(4):
            project(4 * group + member)

        @pl.when((group == 0) & (sp < nsp - 1))
        def _():
            send_right.start()

        @pl.when((group == 0) & (sp > 0))
        def _():
            send_left.start()

        @pl.when(group == 0)
        def _():
            pass_on(near_z)

        return carry

    lax.fori_loop(0, 2, project_group, 0)

    wo_sends[3].wait_recv()
    wo_sends[5].start()
    wo_sends[1].wait_recv()
    wo_sends[2].wait_recv()
    wo_sends[6].start()
    wo_sends[7].start()

    @pl.when(sp > 0)
    def _():
        send_right.wait_recv()

    @pl.when(sp < nsp - 1)
    def _():
        send_left.wait_recv()

    for sample in range(samples):
        store_values(kv_v[sample, :WINDOW].astype(f32).T, sample, ctx)
        store_values(kv_v[sample, WINDOW + tokens :].astype(f32).T, sample, ctx + WINDOW + tokens)
        vt_v[sample, :16, :] = jnp.ones((16, ctx + tokens + 2 * WINDOW), bf16)
    assert nt == 4

    def destination(k):
        late = k // 2
        return lax.rem(tp + (1 - late) * (2 - k) + late * (9 - 3 * k), nt)

    def att_copy(step_k, sample):
        dest = destination(step_k)
        return remote(
            att_v.at[sample, pl.ds(pl.multiple_of(dest * chunk, chunk), chunk), :], by_v.at[tp, sample],
            att_send.at[step_k, sample], att_recv.at[step_k, sample], place(tp_to=dest),
        )

    for load, ref, line in ((small[4], lift_ref, 0), (small[3], sink_ref, 1)):
        load.wait()
        for h in range(4):
            limits_v[line : line + 1, h * WINDOW : (h + 1) * WINDOW] = jnp.broadcast_to(
                ref[0:1, h : h + 1] * LOG2E, (1, WINDOW)
            )
    subs = chunk // WINDOW
    deep_keys = min(256, ctx)
    pieces = [("far", c * deep_keys, c * deep_keys, deep_keys) for c in range(ctx // deep_keys)]
    pieces += [("near", c * WINDOW, ctx + c * WINDOW, WINDOW) for c in range(3)]
    buffers = ((s0_v, t0_v), (s1_v, t1_v))

    def rows_of(step, sub):
        k, sample = step // samples, step % samples
        dest = destination(k)
        return sample, pl.multiple_of(dest * chunk + sub * WINDOW, WINDOW)

    def scores(step, buffer, sub):
        sample, row = rows_of(step, sub)
        left_off = jnp.where((sp == 0) & (row == 0), NEGATIVE, 0.0)
        right_off = jnp.where((sp == nsp - 1) & (row == tokens - WINDOW), NEGATIVE, 0.0)
        score_ref, top_ref = buffer
        return Scores((kv_v, ckv_v, q_v, limits_v), sample, row, left_off, right_off, score_ref.at[sub], top_ref.at[sub])

    def weights(step, buffer, sub):
        sample, row = rows_of(step, sub)
        score_ref, top_ref = buffer
        return Weights(vt_v, limits_v, att_v, ctx, sample, row, score_ref.at[sub], top_ref.at[sub])

    def both(now, later, only="all"):
        for piece in pieces:
            for sub in range(subs):
                if now and only == "all":
                    now[sub].piece(*piece)
                if later and only in ("all", piece[0]):
                    later[sub].piece(*piece)
        for sub in range(subs if only in ("all", None) else 0):
            if later:
                later[sub].done()
            if now:
                now[sub].done()

    start = [scores(0, buffers[0], sub) for sub in range(subs)]
    both(None, start, "near")

    for offset in far_z:
        ctx_along_z(offset).wait_recv()
    drain(ckv_v.at[:, pl.ds(0, nz * (nx - 1))], stage_sem.at[7])
    for sample in range(samples):
        store_values(ckv_v[sample].reshape(ctx, LANES).astype(f32).T, sample, 0)

    both(None, start, "far")
    both(None, start, None)
    turns = nt * samples

    def chunk_step(step, carry):
        for parity in range(2):

            @pl.when(step % 2 == parity)
            def _():
                both(
                    [weights(step, buffers[parity], sub) for sub in range(subs)],
                    [scores(step + 1, buffers[1 - parity], sub) for sub in range(subs)],
                )

        k, sample = step // samples, step % samples

        @pl.when(k < nt - 1)
        def _():
            att_copy(k, sample).start()

        @pl.when(step == 3)
        def _():
            wo_sends[4].wait_recv()
            wo_sends[5].wait_recv()
            wo_sends[8].start()

        return carry

    lax.fori_loop(0, turns - 1, chunk_step, 0)
    both([weights(turns - 1, buffers[(turns - 1) % 2], sub) for sub in range(subs)], None)
    by_v[tp] = att_v[:, pl.ds(pl.multiple_of(tp * chunk, chunk), chunk), :]

    for k in (6, 7, 8):
        wo_sends[k].wait_recv()
    wide = width
    for sample in range(samples):
        for k in range(nt - 1):
            att_copy(k, sample).wait_recv()

        def project_out(step, carry):
            cols = pl.ds(pl.multiple_of(step * wide, wide), wide)
            total = jnp.zeros((chunk, wide), f32)
            for t in range(nt):
                total = total + jnp.dot(
                    by_v[t, sample], wo_v[t * own_rows : (t + 1) * own_rows, cols], preferred_element_type=f32
                )
            out_v[sample, :, cols] = (total * modr_v[6 + sample : 7 + sample, cols]).astype(bf16)
            return carry

        lax.fori_loop(0, width // wide, project_out, 0)

    drain(rx_v, stage_sem.at[0])
    drain(rz_v, stage_sem.at[2])
    drain(mod_v.at[pl.ds(0, nt * nx - 1)], stage_sem.at[4])
    drain(ckv_v.at[:, pl.ds(0, nz * (nx - 1))], stage_sem.at[6])
    for offset in range(1, nz):
        ctx_along_z(offset).wait_send()
    for copy in wo_sends:
        copy.wait_send()

    @pl.when(sp < nsp - 1)
    def _():
        send_right.wait_send()

    @pl.when(sp > 0)
    def _():
        send_left.wait_send()

    for k in range(nt - 1):
        for sample in range(samples):
            att_copy(k, sample).wait_send()


def shards(
    sizes, latent, context, condition, ctx_cond, norm_gain, w_shift, w_scale, w_gate, w_query, w_key, w_value, w_out,
    sink_logit, ctx_lift,
):
    nsp, nx, nt, nd = sizes
    nz = nsp // nx
    samples, tokens, width = latent.shape
    ctx_local = context.shape[1]
    ctx = ctx_local * nsp
    feats = condition.shape[1]
    cols = w_shift.shape[1]
    chunk = tokens // nt
    keys = ctx + tokens + 2 * WINDOW
    own_rows = w_out.shape[0]
    anywhere = pl.BlockSpec(memory_space=pltpu.HBM)
    vmem = pl.BlockSpec(memory_space=pltpu.VMEM)
    dma = pltpu.SemaphoreType.DMA
    return pl.pallas_call(
        functools.partial(layer, sizes),
        out_shape=pltpu.VMEM((samples, chunk, width), bf16),
        in_specs=[anywhere] * 14,
        out_specs=vmem,
        scratch_shapes=[
            pltpu.VMEM((samples, feats), bf16),
            pltpu.VMEM((1, feats), bf16),
            pltpu.VMEM((1, width), f32),
            pltpu.VMEM((1, 4), f32),
            pltpu.VMEM((1, 4), f32),
            pltpu.VMEM((samples, tokens, width), bf16),
            pltpu.VMEM((samples, ctx_local, width), bf16),
            pltpu.VMEM((3, feats, cols), bf16),
            pltpu.VMEM((width, 4 * HEAD), bf16),
            pltpu.VMEM((LANES, width), bf16),
            pltpu.VMEM((width, LANES), bf16),
            pltpu.VMEM((own_rows * nt, width), bf16),
            pltpu.VMEM((16, feats), f32),
            pltpu.VMEM((nx, 8, LANES), f32),
            pltpu.VMEM((nx - 1, 8, LANES), f32),
            pltpu.VMEM((8, LANES), f32),
            pltpu.VMEM((nz - 1, 8, LANES), f32),
            pltpu.VMEM((nt * nx, 8, LANES), f32),
            pltpu.VMEM((8, width), f32),
            pltpu.VMEM((samples, 8, width), f32),
            pltpu.VMEM((samples, 8, width), f32),
            pltpu.VMEM((samples, tokens, LANES), f32),
            pltpu.VMEM((tokens, LANES), f32),
            pltpu.VMEM((tokens, LANES), f32),
            pltpu.VMEM((samples, tokens, 4 * HEAD), bf16),
            pltpu.VMEM((samples, tokens + 2 * WINDOW, LANES), bf16),
            pltpu.VMEM((samples, nsp, ctx_local, LANES), bf16),
            pltpu.VMEM((samples, HEAD + 16, keys), bf16),
            pltpu.VMEM((8, 4 * WINDOW), f32),
            pltpu.VMEM((chunk // WINDOW, ctx + 3 * WINDOW, 4 * WINDOW), f32),
            pltpu.VMEM((chunk // WINDOW, ctx + 3 * WINDOW, 4 * WINDOW), f32),
            pltpu.VMEM((chunk // WINDOW, 8, 4 * WINDOW), f32),
            pltpu.VMEM((chunk // WINDOW, 8, 4 * WINDOW), f32),
            pltpu.VMEM((samples, tokens, 2 * LANES), bf16),
            pltpu.VMEM((nt, samples, chunk, 2 * LANES), bf16),
            dma((14,)),
            dma((8,)),
            dma((2, nz)),
            dma((2,)),
            dma((2,)),
            dma((9,)),
            dma((9,)),
            dma((nt - 1, samples)),
            dma((nt - 1, samples)),
        ],
        compiler_params=pltpu.CompilerParams(
            collective_id=0, has_side_effects=True, vmem_limit_bytes=61 * 1024 * 1024
        ),
        name="layer",
    )(
        latent, context, condition, ctx_cond.reshape(1, feats), norm_gain.reshape(1, width), w_shift, w_scale, w_gate,
        w_query, w_key.T, w_value.T, w_out, sink_logit.reshape(1, 4), ctx_lift.reshape(1, 4),
    )


def solution(mesh):
    nsp, nt, nd = mesh.shape["sp"], mesh.shape["tp"], mesh.shape["dp"]
    sizes = (nsp, 4 if nsp > 4 else 2, nt, nd)
    return jax.shard_map(
        functools.partial(shards, sizes),
        mesh=mesh,
        in_specs=(
            P("dp", "sp", None),
            P("dp", "sp", None),
            P("dp", "sp"),
            P("sp"),
            P(),
            P("sp", "tp"),
            P("sp", "tp"),
            P("sp", "tp"),
            P(None, "tp"),
            P(None, "tp"),
            P(None, "tp"),
            P("tp", None),
            P("tp"),
            P("tp"),
        ),
        out_specs=P("dp", ("sp", "tp"), None),
        check_vma=False,
    )
```

```python
import functools
import math

import jax
import jax.numpy as jnp
from jax import lax
from jax.experimental import pallas as pl
from jax.experimental.pallas import tpu as pltpu
from jax.sharding import PartitionSpec as P

HEAD = 64
WINDOW = 128
GRID_COLS = 64
EPSILON = 1e-06
ROPE_BASE = 10000.0
NEGATIVE = -1e30
LOG2E = math.log2(math.e)
LANES = 128
MESH = pl.DeviceIdType.MESH
f32 = jnp.float32
bf16 = jnp.bfloat16


def lanes_of(rows):
    return lax.broadcasted_iota(jnp.int32, (rows, LANES), 1)


def drain(ref, sem):
    pltpu.make_async_copy(ref, ref, sem).wait()


def swapped(u, lane):
    return jnp.where(lane % 32 < 16, pltpu.roll(u, LANES - 16, 1), pltpu.roll(u, 16, 1))


class Scores:
    def __init__(self, kv, ckv, q_ref, sample, row):
        self.kv, self.ckv, self.sample, self.row = kv, ckv, sample, row
        turned = q_ref[sample, pl.ds(row, WINDOW), :].astype(f32).T.astype(bf16)
        self.q = jnp.concatenate([turned[h * HEAD : (h + 1) * HEAD] for h in range(4)], axis=1)
        self.top = None

    def put(self, score, score_ref, at):
        rows = score.shape[0]
        score_ref[at : at + rows, :] = score
        top = jnp.max(score.reshape(rows // 8, 8, score.shape[1]), axis=0)
        self.top = top if self.top is None else jnp.maximum(self.top, top)

    def far(self, at, rows, score_ref):
        local = self.ckv.shape[2]
        keys = self.ckv[self.sample, at // local : (at + rows) // local].reshape(rows, LANES)
        self.put(jnp.dot(keys[:, :HEAD], self.q, preferred_element_type=f32), score_ref, at)

    def near(self, at, score_ref, offset):
        keys = self.kv[self.sample, pl.ds(pl.multiple_of(self.row + at, WINDOW), WINDOW), :]
        score = jnp.dot(keys[:, :HEAD], self.q, preferred_element_type=f32)
        if at != WINDOW:
            key = lax.broadcasted_iota(jnp.int32, score.shape, 0)
            query = lax.broadcasted_iota(jnp.int32, score.shape, 1) % WINDOW
            inside = key >= query if at == 0 else key <= query
            score = jnp.where(inside, score, NEGATIVE) + offset
        self.put(score, score_ref, at)


class Weights:
    def __init__(self, vt, limits, att, ctx, sample, row, score_ref, near_ref, top_ref):
        self.vt, self.att, self.ctx, self.sample, self.row, self.score_ref = vt, att, ctx, sample, row, score_ref
        self.near_ref = near_ref
        self.top = top_ref[0:1, :]
        self.lowered = self.top - limits[0:1, :]
        self.sink = jnp.exp2(limits[1:2, :] - self.top)
        self.total = jnp.zeros((vt.shape[1], 4 * WINDOW), f32)

    def piece(self, kind, at, rows):
        if kind == "far":
            score, top = self.score_ref[at : at + rows, :], self.lowered
            values = self.vt[self.sample, :, at : at + rows]
        else:
            score, top = self.near_ref[at : at + rows, :], self.top
            values = self.vt[self.sample, :, pl.ds(pl.multiple_of(self.ctx + self.row + at, WINDOW), rows)]
        weight = jnp.exp2(score - top).astype(bf16)
        self.total = self.total + jnp.dot(values, weight, preferred_element_type=f32)

    def done(self):
        out = self.total[16:] * (1.0 / (self.total[0:1] + self.sink))
        stacked = jnp.concatenate([out[:, h * WINDOW : (h + 1) * WINDOW] for h in range(4)], axis=0)
        self.att[self.sample, pl.ds(self.row, WINDOW), :] = stacked.T.astype(bf16)


def gated(by_v, wo_v, modr_v, sample, cols):
    owners = by_v.shape[0]
    rows = wo_v.shape[0] // owners
    total = jnp.zeros((by_v.shape[2], modr_v[0:1, cols].shape[1]), f32)
    for t in range(owners):
        total = total + jnp.dot(
            by_v[t, sample], wo_v[t * rows : (t + 1) * rows, cols], preferred_element_type=f32
        )
    return (total * modr_v[6 + sample : 7 + sample, cols]).astype(bf16)


def closing(first_v, by_v, wo_v, modr_v, out_hbm, last_v, sem):
    copies = [pltpu.make_async_copy(first_v, out_hbm.at[0], sem.at[0])]
    copies[0].start()
    wide = last_v.shape[1] // 4
    for n in range(4):
        cols = slice(n * wide, (n + 1) * wide)
        last_v[:, cols] = gated(by_v, wo_v, modr_v, 1, cols)
        copies.append(pltpu.make_async_copy(last_v.at[:, cols], out_hbm.at[1, :, cols], sem.at[1 + n]))
        copies[-1].start()
    for copy in copies:
        copy.wait()


def layer(
    sizes,
    x_hbm, context_hbm, condition_hbm, ctx_cond_hbm, gain_hbm, wsh_hbm, wsc_hbm, wga_hbm, wq_hbm, wk_hbm, wv_hbm, wo_hbm,
    sink_hbm, lift_hbm,
    out_v, by_v, wo_v, modr_v,
    condition, ctx_cond, gain, sink_ref, lift_ref, x_v, context_v, wm_v, wq_v, wt_v, wkv_v,
    active_v, part_v, rx_v, zsrc_v, rz_v, mod_v, mul_v, add_v,
    inv_v, cos_v, sin_v, q_v, kv_v, ckv_v, vt_v, limits_v, near_v, near_top_v, s0_v, s1_v, t0_v, t1_v, att_v,
    local_sem, stage_sem, ctx_sem, halo_send, halo_recv, wo_send, wo_recv, att_send, att_recv,
):
    nsp, nx, nt, nd = sizes
    nz = nsp // nx
    samples, tokens, width = x_v.shape
    chunk = tokens // nt
    ctx_local = context_v.shape[1]
    ctx = ctx_local * nsp
    sp = lax.axis_index("sp")
    tp = lax.axis_index("tp")
    dp = lax.axis_index("dp")
    xi = lax.rem(sp, nx)
    zi = lax.div(sp, nx)

    def place(sp_to=None, tp_to=None, dp_to=None):
        return {
            "sp": sp if sp_to is None else sp_to,
            "tp": tp if tp_to is None else tp_to,
            "dp": dp if dp_to is None else dp_to,
        }

    def remote(src, dst, send, recv, device):
        return pltpu.make_async_remote_copy(
            src_ref=src, dst_ref=dst, send_sem=send, recv_sem=recv, device_id=device, device_id_type=MESH
        )

    def x_peer(offset):
        return zi * nx + lax.rem(xi + offset, nx)

    def z_peer(offset):
        return lax.rem(zi + offset, nz) * nx + xi

    own_rows = wo_hbm.shape[0]
    half = own_rows // nd
    loads = [
        pltpu.make_async_copy(wsh_hbm, wm_v.at[0], local_sem.at[0]),
        pltpu.make_async_copy(wsc_hbm, wm_v.at[1], local_sem.at[1]),
        pltpu.make_async_copy(wga_hbm, wm_v.at[2], local_sem.at[2]),
        pltpu.make_async_copy(
            wo_hbm, wo_v.at[pl.ds(pl.multiple_of(tp * own_rows, own_rows), own_rows), :], local_sem.at[3]
        ),
        pltpu.make_async_copy(context_hbm, context_v, local_sem.at[4]),
        pltpu.make_async_copy(x_hbm, x_v, local_sem.at[5]),
        pltpu.make_async_copy(wk_hbm, wt_v.at[pl.ds(0, HEAD), :], local_sem.at[6]),
        pltpu.make_async_copy(wv_hbm, wt_v.at[pl.ds(HEAD, HEAD), :], local_sem.at[7]),
        pltpu.make_async_copy(wq_hbm, wq_v, local_sem.at[8]),
    ]
    small = [
        pltpu.make_async_copy(condition_hbm, condition, local_sem.at[9]),
        pltpu.make_async_copy(ctx_cond_hbm, ctx_cond, local_sem.at[10]),
        pltpu.make_async_copy(gain_hbm, gain, local_sem.at[11]),
        pltpu.make_async_copy(sink_hbm, sink_ref, local_sem.at[12]),
        pltpu.make_async_copy(lift_hbm, lift_ref, local_sem.at[13]),
    ]
    for load in small[:2] + loads[:3] + loads[6:8] + loads[3:5] + loads[8:] + small[2:] + loads[5:6]:
        load.start()

    barrier = pltpu.get_barrier_semaphore()

    def greet(device):
        pl.semaphore_signal(barrier, inc=1, device_id=device, device_id_type=MESH)

    for offset in range(1, nx):
        greet(place(sp_to=x_peer(offset)))
    for offset in range(1, nz):
        greet(place(sp_to=z_peer(offset)))
    for offset in range(1, nt):
        greet(place(tp_to=lax.rem(tp + offset, nt)))
    for offset in range(1, nd):
        greet(place(dp_to=lax.rem(dp + offset, nd)))

    active_v[...] = jnp.zeros_like(active_v)
    for load in small[:2]:
        load.wait()
    active_v[0:2, :] = condition[...].astype(f32)
    active_v[2:3, :] = ctx_cond[...].astype(f32)
    raw = active_v[...]
    active = (raw / (1.0 + jnp.exp(-raw))).astype(bf16)
    for load in loads[:3]:
        load.wait()
    vecs = [jnp.dot(active, wm_v[k], preferred_element_type=f32) for k in range(3)]
    for c in range(nx):
        cols = slice(c * LANES, (c + 1) * LANES)
        part_v[c, 0:3, :] = vecs[0][0:3, cols]
        part_v[c, 3:6, :] = vecs[1][0:3, cols]
        part_v[c, 6:8, :] = vecs[2][0:2, cols]

    pl.semaphore_wait(barrier, (nx - 1) + (nz - 1) + (nt - 1) + (nd - 1))

    for offset in range(1, nx):
        to = lax.rem(xi + offset, nx)
        remote(part_v.at[to], rx_v.at[offset - 1], stage_sem.at[0], stage_sem.at[1], place(sp_to=x_peer(offset))).start()

    loads[3].wait()

    def wo_rows(owner, core, start, count):
        return wo_v.at[pl.ds(pl.multiple_of(owner * own_rows + core * half + start, count), count), :]

    after = lax.rem(tp + 1, nt)
    before = lax.rem(tp + nt - 1, nt)
    across = lax.rem(tp + 2, nt)
    other = lax.rem(dp + 1, nd)
    quarter = half // 2

    def wo_copy(k, ref, device):
        return remote(ref, ref, wo_send.at[k], wo_recv.at[k], device)

    wo_sends = [
        wo_copy(0, wo_rows(tp, dp, 0, quarter), place(tp_to=after)),
        wo_copy(1, wo_rows(tp, dp, 0, quarter), place(tp_to=before)),
        wo_copy(2, wo_rows(tp, dp, quarter, quarter), place(tp_to=after)),
        wo_copy(3, wo_rows(tp, dp, quarter, quarter), place(tp_to=before)),
        wo_copy(4, wo_rows(before, dp, 0, quarter), place(tp_to=after)),
        wo_copy(5, wo_rows(after, dp, quarter, quarter), place(tp_to=before)),
        wo_copy(6, wo_rows(before, dp, 0, half), place(dp_to=other)),
        wo_copy(7, wo_rows(after, dp, 0, half), place(dp_to=other)),
        wo_copy(8, wo_rows(across, dp, 0, half), place(dp_to=other)),
    ]
    wo_sends[0].start()
    wo_sends[1].start()

    block = min(256, chunk)
    blocks = tokens // block

    def statistics(step):
        sample, start = step // blocks, pl.multiple_of(step % blocks * block, block)
        total = jnp.zeros((block, LANES), f32)
        for c in range(width // LANES):
            piece = x_v[sample, pl.ds(start, block), c * LANES : (c + 1) * LANES].astype(f32)
            total = total + piece * piece
        mean = jnp.sum(total, axis=1, keepdims=True) / width
        inv_v[sample, pl.ds(start, block), :] = jnp.broadcast_to(lax.rsqrt(mean + EPSILON), (block, LANES))

    def stats_loop(first, last):
        def run(step, carry):
            statistics(step)
            return carry

        lax.fori_loop(first, last, run, 0)

    all_blocks = samples * blocks
    loads[6].wait()
    loads[7].wait()
    wkv_v[...] = wt_v[...].T
    lane1 = lanes_of(8)
    frequency = jnp.exp((lane1[0:1] % 16).astype(f32) * (-math.log(ROPE_BASE) / 16.0))
    grid_rows = tokens // GRID_COLS
    table_rows = max(grid_rows, 8)
    row_pos = (sp * grid_rows + lax.broadcasted_iota(jnp.int32, (table_rows, LANES), 0)).astype(f32)
    col_pos = lax.broadcasted_iota(jnp.int32, (GRID_COLS, LANES), 0).astype(f32)
    row_cos, row_sin = jnp.cos(row_pos * frequency), jnp.sin(row_pos * frequency)
    col_cos, col_sin = jnp.cos(col_pos * frequency), jnp.sin(col_pos * frequency)
    lane64 = lanes_of(GRID_COLS)
    by_row = lane64 % HEAD < 32
    minus = lane64 % 32 < 16
    for t in range(grid_rows):
        rows = slice(t * GRID_COLS, (t + 1) * GRID_COLS)
        cos_v[rows, :] = jnp.where(by_row, row_cos[t : t + 1, :], col_cos)
        sine = jnp.where(by_row, row_sin[t : t + 1, :], col_sin)
        sin_v[rows, :] = jnp.where(minus, -sine, sine)

    drain(rx_v, stage_sem.at[1])
    quarter_sum = part_v[xi]
    for k in range(nx - 1):
        quarter_sum = quarter_sum + rx_v[k]
    zsrc_v[...] = quarter_sum

    for offset in range(1, nz):
        remote(zsrc_v, rz_v.at[offset - 1], stage_sem.at[2], stage_sem.at[3], place(sp_to=z_peer(offset))).start()

    loads[5].wait()
    stats_loop(0, all_blocks // 2)
    drain(rz_v, stage_sem.at[3])
    total = zsrc_v[...]
    for k in range(nz - 1):
        total = total + rz_v[k]
    here = tp * nx + xi
    mod_v[here] = total

    for dy in range(nt):
        for dx in range(nx):
            if dy or dx:
                remote(
                    mod_v.at[here], mod_v.at[here], stage_sem.at[4], stage_sem.at[5],
                    place(sp_to=x_peer(dx), tp_to=lax.rem(tp + dy, nt)),
                ).start()

    wo_sends[2].start()
    wo_sends[3].start()
    wo_sends[0].wait_recv()
    wo_sends[4].start()

    @pl.when(sp == 0)
    def _():
        kv_v[:, 0:WINDOW, :] = jnp.zeros((samples, WINDOW, LANES), bf16)

    @pl.when(sp == nsp - 1)
    def _():
        kv_v[:, WINDOW + tokens :, :] = jnp.zeros((samples, WINDOW, LANES), bf16)

    loads[4].wait()
    loads[8].wait()
    ctx_rows = samples * ctx_local
    ctx_wide = context_v[...].reshape(ctx_rows, width).astype(f32)
    ctx_inv = lax.rsqrt(jnp.mean(ctx_wide * ctx_wide, axis=1, keepdims=True) + EPSILON)
    ctx_unit = ctx_wide * ctx_inv

    stats_loop(all_blocks // 2, all_blocks)
    drain(mod_v.at[pl.ds(0, nt * nx - 1)], stage_sem.at[5])
    for k in range(nt * nx):
        modr_v[:, k * LANES : (k + 1) * LANES] = mod_v[k]
    small[2].wait()
    scaled = gain[...] * (1.0 + modr_v[3:6, :])
    for r in range(samples):
        mul_v[r, 0:1, :] = scaled[r : r + 1]
        add_v[r, 0:1, :] = modr_v[r : r + 1, :]

    ctx_hidden = (ctx_unit * scaled[2:3] + modr_v[2:3, :]).astype(bf16)
    ctx_pairs = jnp.dot(ctx_hidden, wkv_v[...], preferred_element_type=f32).astype(bf16)
    ckv_v[:, pl.ds(sp, 1)] = ctx_pairs.reshape(samples, 1, ctx_local, LANES)

    def ctx_rows_of(owner):
        return ckv_v.at[:, pl.ds(owner, 1)]

    def ctx_along_x(owner_z):
        rows = ctx_rows_of(owner_z * nx + xi)
        for offset in range(1, nx):
            remote(rows, rows, stage_sem.at[6], stage_sem.at[7], place(sp_to=x_peer(offset))).start()

    def ctx_along_z(offset):
        rows = ctx_rows_of(sp)
        return remote(rows, rows, ctx_sem.at[0, offset], ctx_sem.at[1, offset], place(sp_to=z_peer(offset)))

    far_z = [nz // 2]
    near_z = [offset for offset in range(1, nz) if min(offset, nz - offset) < min(3, nz // 2)]
    mid_z = [offset for offset in range(1, nz) if offset not in near_z + far_z]
    for offset in near_z + mid_z:
        ctx_along_z(offset).start()
    ctx_along_x(zi)
    own_pairs = ctx_rows_of(sp)
    for offset in far_z:
        ctx_along_z(offset).start()
        for dx in range(1, nx):
            to = lax.rem(zi + offset, nz) * nx + lax.rem(xi + dx, nx)
            remote(own_pairs, own_pairs, stage_sem.at[6], stage_sem.at[7], place(sp_to=to)).start()

    def pass_on(offsets):
        for offset in offsets:
            ctx_along_z(offset).wait_recv()
            ctx_along_x(lax.rem(zi + nz - offset, nz))

    lane = lanes_of(block)
    low = lane < HEAD

    assert blocks == 4 and samples == 2
    steps = 4
    deep = width // steps
    factor = HEAD ** (-0.5) * LOG2E

    def block_of(step):
        late, turn = step // 4, step % 4
        index = (1 - late) * (turn % 2) * (blocks - 1) + late * (1 + turn % 2)
        return turn // 2, pl.multiple_of(index * block, block)

    def store_values(pairs_t, sample, start):
        vt_v[sample, 16:, pl.ds(start, pairs_t.shape[1])] = pairs_t[HEAD:].astype(bf16)

    def project(step):
        sample, start = block_of(step)
        inverse = inv_v[sample, pl.ds(start, block), :]
        q_acc = jnp.zeros((block, 2 * LANES), f32)
        kv_acc = jnp.zeros((block, LANES), f32)
        for k in range(steps):
            hidden = []
            for c in range(deep // LANES):
                cols = slice(k * deep + c * LANES, k * deep + (c + 1) * LANES)
                wide = x_v[sample, pl.ds(start, block), cols].astype(f32)
                hidden.append((wide * inverse * mul_v[sample, 0:1, cols] + add_v[sample, 0:1, cols]).astype(bf16))
            hidden = jnp.concatenate(hidden, axis=1)
            q_acc = q_acc + jnp.dot(hidden, wq_v[k * deep : (k + 1) * deep, :], preferred_element_type=f32)
            kv_acc = kv_acc + jnp.dot(hidden, wkv_v[k * deep : (k + 1) * deep, :], preferred_element_type=f32)
        cosine = cos_v[pl.ds(start, block), :]
        sine = sin_v[pl.ds(start, block), :]
        turned = jnp.where(low, kv_acc * cosine + swapped(kv_acc, lane) * sine, kv_acc)
        kv_v[sample, pl.ds(pl.multiple_of(WINDOW + start, WINDOW), block), :] = turned.astype(bf16)
        store_values(turned.T, sample, pl.multiple_of(ctx + WINDOW + start, WINDOW))
        for pair in range(2):
            u = q_acc[:, pair * LANES : (pair + 1) * LANES]
            turned = (u * cosine + swapped(u, lane) * sine) * factor
            q_v[sample, pl.ds(start, block), pair * LANES : (pair + 1) * LANES] = turned.astype(bf16)

    send_right = remote(
        kv_v.at[:, pl.ds(tokens, WINDOW), :], kv_v.at[:, pl.ds(0, WINDOW), :], halo_send.at[0], halo_recv.at[0],
        place(sp_to=lax.rem(sp + 1, nsp)),
    )
    send_left = remote(
        kv_v.at[:, pl.ds(WINDOW, WINDOW), :], kv_v.at[:, pl.ds(WINDOW + tokens, WINDOW), :], halo_send.at[1],
        halo_recv.at[1], place(sp_to=lax.rem(sp + nsp - 1, nsp)),
    )

    def project_some(first, count):
        def run(group, carry):
            for member in range(count):
                project(first + count * group + member)
            return carry

        lax.fori_loop(0, 1, run, 0)

    project_some(0, 4)

    @pl.when(sp < nsp - 1)
    def _():
        send_right.start()

    @pl.when(sp > 0)
    def _():
        send_left.start()

    project_some(4, 2)
    pass_on(near_z)
    wo_sends[3].wait_recv()
    wo_sends[5].start()
    project_some(6, 2)
    pass_on(mid_z)

    assert nt == 4

    def destination(k):
        late = k // 2
        return lax.rem(tp + (1 - late) * (2 - k) + late * (9 - 3 * k), nt)

    def att_copy(step_k, sample):
        dest = destination(step_k)
        return remote(
            att_v.at[sample, pl.ds(pl.multiple_of(dest * chunk, chunk), chunk), :], by_v.at[tp, sample],
            att_send.at[step_k, sample], att_recv.at[step_k, sample], place(tp_to=dest),
        )

    for load, ref, line in ((small[4], lift_ref, 0), (small[3], sink_ref, 1)):
        load.wait()
        for h in range(4):
            limits_v[line : line + 1, h * WINDOW : (h + 1) * WINDOW] = jnp.broadcast_to(
                ref[0:1, h : h + 1] * LOG2E, (1, WINDOW)
            )
    subs = chunk // WINDOW
    deep_keys = min(256, ctx)
    pieces = [("far", c * deep_keys, deep_keys) for c in range(ctx // deep_keys)]
    pieces += [("near", c * WINDOW, WINDOW) for c in range(3)]
    buffers = ((s0_v, t0_v), (s1_v, t1_v))

    def rows_of(step, sub):
        k, sample = step // samples, step % samples
        dest = destination(k)
        return sample, pl.multiple_of(dest * chunk + sub * WINDOW, WINDOW)

    def near_scores(sample, dest):
        place_of = dest * samples + sample
        for sub in range(subs):
            row = pl.multiple_of(dest * chunk + sub * WINDOW, WINDOW)
            left_off = jnp.where((sp == 0) & (row == 0), NEGATIVE, 0.0)
            right_off = jnp.where((sp == nsp - 1) & (row == tokens - WINDOW), NEGATIVE, 0.0)
            score = Scores(kv_v, ckv_v, q_v, sample, row)
            for at, offset in ((0, left_off), (WINDOW, 0.0), (2 * WINDOW, right_off)):
                score.near(at, near_v.at[place_of, sub], offset)
            near_top_v[place_of, sub] = score.top

    def near_of(step):
        k, sample = step // samples, step % samples
        return destination(k) * samples + sample

    def near_pair(first, apart):
        def run(turn, carry):
            for sample in range(samples):
                near_scores(sample, first + apart * turn)
            return carry

        lax.fori_loop(0, 2, run, 0)

    near_pair(1, 1)

    @pl.when(sp > 0)
    def _():
        send_right.wait_recv()

    @pl.when(sp < nsp - 1)
    def _():
        send_left.wait_recv()

    for sample in range(samples):
        store_values(kv_v[sample, :WINDOW].astype(f32).T, sample, ctx)
        store_values(kv_v[sample, WINDOW + tokens :].astype(f32).T, sample, ctx + WINDOW + tokens)
        vt_v[sample, :16, :] = jnp.ones((16, ctx + tokens + 2 * WINDOW), bf16)
    near_pair(0, nt - 1)

    for offset in far_z:
        ctx_along_z(offset).wait_recv()
    drain(ckv_v.at[:, pl.ds(0, nz * (nx - 1))], stage_sem.at[7])
    for sample in range(samples):
        store_values(ckv_v[sample].reshape(ctx, LANES).astype(f32).T, sample, 0)


    def scores(step, sub):
        sample, row = rows_of(step, sub)
        return Scores(kv_v, ckv_v, q_v, sample, row)

    def weights(step, buffer, sub):
        sample, row = rows_of(step, sub)
        score_ref, top_ref = buffer
        return Weights(
            vt_v, limits_v, att_v, ctx, sample, row, score_ref.at[sub], near_v.at[near_of(step), sub], top_ref.at[sub]
        )

    def both(now, later, step, buffer):
        for kind, at, rows in pieces:
            for sub in range(subs):
                if now:
                    now[sub].piece(kind, at, rows)
                if later and kind == "far":
                    later[sub].far(at, rows, buffer[0].at[sub])
        for sub in range(subs):
            if later:
                far = jnp.max(later[sub].top, axis=0, keepdims=True) + limits_v[0:1, :]
                near = jnp.max(near_top_v[near_of(step), sub], axis=0, keepdims=True)
                buffer[1][sub, 0:1, :] = jnp.maximum(jnp.maximum(far, near), limits_v[1:2, :])
            if now:
                now[sub].done()

    both(None, [scores(0, sub) for sub in range(subs)], 0, buffers[0])
    turns = nt * samples

    def chunk_step(step, carry):
        for parity in range(2):

            @pl.when(step % 2 == parity)
            def _():
                both(
                    [weights(step, buffers[parity], sub) for sub in range(subs)],
                    [scores(step + 1, sub) for sub in range(subs)],
                    step + 1,
                    buffers[1 - parity],
                )

        k, sample = step // samples, step % samples

        @pl.when(k < nt - 1)
        def _():
            att_copy(k, sample).start()

        @pl.when(step == 1)
        def _():
            wo_sends[1].wait_recv()
            wo_sends[2].wait_recv()
            wo_sends[6].start()
            wo_sends[7].start()

        @pl.when(step == 3)
        def _():
            wo_sends[4].wait_recv()
            wo_sends[5].wait_recv()
            wo_sends[8].start()

        return carry

    lax.fori_loop(0, turns - 1, chunk_step, 0)
    both([weights(turns - 1, buffers[(turns - 1) % 2], sub) for sub in range(subs)], None, None, None)
    by_v[tp] = att_v[:, pl.ds(pl.multiple_of(tp * chunk, chunk), chunk), :]

    for k in (6, 7, 8):
        wo_sends[k].wait_recv()
    for k in range(nt - 1):
        att_copy(k, 0).wait_recv()
    out_v[...] = gated(by_v, wo_v, modr_v, 0, slice(0, width))
    for sample in range(1, samples):
        for k in range(nt - 1):
            att_copy(k, sample).wait_recv()

    drain(rx_v, stage_sem.at[0])
    drain(rz_v, stage_sem.at[2])
    drain(mod_v.at[pl.ds(0, nt * nx - 1)], stage_sem.at[4])
    drain(ckv_v.at[:, pl.ds(0, nz * (nx - 1))], stage_sem.at[6])
    for offset in range(1, nz):
        ctx_along_z(offset).wait_send()
    for copy in wo_sends:
        copy.wait_send()

    @pl.when(sp < nsp - 1)
    def _():
        send_right.wait_send()

    @pl.when(sp > 0)
    def _():
        send_left.wait_send()

    for k in range(nt - 1):
        for sample in range(samples):
            att_copy(k, sample).wait_send()


def shards(
    sizes, latent, context, condition, ctx_cond, norm_gain, w_shift, w_scale, w_gate, w_query, w_key, w_value, w_out,
    sink_logit, ctx_lift,
):
    nsp, nx, nt, nd = sizes
    nz = nsp // nx
    samples, tokens, width = latent.shape
    ctx_local = context.shape[1]
    ctx = ctx_local * nsp
    feats = condition.shape[1]
    cols = w_shift.shape[1]
    chunk = tokens // nt
    keys = ctx + tokens + 2 * WINDOW
    own_rows = w_out.shape[0]
    anywhere = pl.BlockSpec(memory_space=pltpu.HBM)
    vmem = pl.BlockSpec(memory_space=pltpu.VMEM)
    dma = pltpu.SemaphoreType.DMA
    kept = pl.pallas_call(
        functools.partial(layer, sizes),
        out_shape=(
            pltpu.VMEM((chunk, width), bf16),
            pltpu.VMEM((nt, samples, chunk, 2 * LANES), bf16),
            pltpu.VMEM((own_rows * nt, width), bf16),
            pltpu.VMEM((8, width), f32),
        ),
        in_specs=[anywhere] * 14,
        out_specs=(vmem,) * 4,
        scratch_shapes=[
            pltpu.VMEM((samples, feats), bf16),
            pltpu.VMEM((1, feats), bf16),
            pltpu.VMEM((1, width), f32),
            pltpu.VMEM((1, 4), f32),
            pltpu.VMEM((1, 4), f32),
            pltpu.VMEM((samples, tokens, width), bf16),
            pltpu.VMEM((samples, ctx_local, width), bf16),
            pltpu.VMEM((3, feats, cols), bf16),
            pltpu.VMEM((width, 4 * HEAD), bf16),
            pltpu.VMEM((LANES, width), bf16),
            pltpu.VMEM((width, LANES), bf16),
            pltpu.VMEM((16, feats), f32),
            pltpu.VMEM((nx, 8, LANES), f32),
            pltpu.VMEM((nx - 1, 8, LANES), f32),
            pltpu.VMEM((8, LANES), f32),
            pltpu.VMEM((nz - 1, 8, LANES), f32),
            pltpu.VMEM((nt * nx, 8, LANES), f32),
            pltpu.VMEM((samples, 8, width), f32),
            pltpu.VMEM((samples, 8, width), f32),
            pltpu.VMEM((samples, tokens, LANES), f32),
            pltpu.VMEM((tokens, LANES), f32),
            pltpu.VMEM((tokens, LANES), f32),
            pltpu.VMEM((samples, tokens, 4 * HEAD), bf16),
            pltpu.VMEM((samples, tokens + 2 * WINDOW, LANES), bf16),
            pltpu.VMEM((samples, nsp, ctx_local, LANES), bf16),
            pltpu.VMEM((samples, HEAD + 16, keys), bf16),
            pltpu.VMEM((8, 4 * WINDOW), f32),
            pltpu.VMEM((nt * samples, chunk // WINDOW, 3 * WINDOW, 4 * WINDOW), f32),
            pltpu.VMEM((nt * samples, chunk // WINDOW, 8, 4 * WINDOW), f32),
            pltpu.VMEM((chunk // WINDOW, ctx, 4 * WINDOW), f32),
            pltpu.VMEM((chunk // WINDOW, ctx, 4 * WINDOW), f32),
            pltpu.VMEM((chunk // WINDOW, 8, 4 * WINDOW), f32),
            pltpu.VMEM((chunk // WINDOW, 8, 4 * WINDOW), f32),
            pltpu.VMEM((samples, tokens, 2 * LANES), bf16),
            dma((14,)),
            dma((8,)),
            dma((2, nz)),
            dma((2,)),
            dma((2,)),
            dma((9,)),
            dma((9,)),
            dma((nt - 1, samples)),
            dma((nt - 1, samples)),
        ],
        compiler_params=pltpu.CompilerParams(
            collective_id=0, has_side_effects=True, vmem_limit_bytes=56 * 1024 * 1024
        ),
        name="layer",
    )(
        latent, context, condition, ctx_cond.reshape(1, feats), norm_gain.reshape(1, width), w_shift, w_scale, w_gate,
        w_query, w_key.T, w_value.T, w_out, sink_logit.reshape(1, 4), ctx_lift.reshape(1, 4),
    )
    return pl.pallas_call(
        closing,
        out_shape=jax.ShapeDtypeStruct((samples, chunk, width), bf16),
        in_specs=[vmem] * 4,
        out_specs=anywhere,
        scratch_shapes=[pltpu.VMEM((chunk, width), bf16), dma((5,))],
        compiler_params=pltpu.CompilerParams(vmem_limit_bytes=16 * 1024 * 1024),
        name="closing",
    )(*kept)


def solution(mesh):
    nsp, nt, nd = mesh.shape["sp"], mesh.shape["tp"], mesh.shape["dp"]
    sizes = (nsp, 4 if nsp > 4 else 2, nt, nd)
    return jax.shard_map(
        functools.partial(shards, sizes),
        mesh=mesh,
        in_specs=(
            P("dp", "sp", None),
            P("dp", "sp", None),
            P("dp", "sp"),
            P("sp"),
            P(),
            P("sp", "tp"),
            P("sp", "tp"),
            P("sp", "tp"),
            P(None, "tp"),
            P(None, "tp"),
            P(None, "tp"),
            P("tp", None),
            P("tp"),
            P("tp"),
        ),
        out_specs=P("dp", ("sp", "tp"), None),
        check_vma=False,
    )
```

```python
import functools
import math

import jax
import jax.numpy as jnp
from jax import lax
from jax.experimental import pallas as pl
from jax.experimental.pallas import tpu as pltpu
from jax.sharding import PartitionSpec as P

HEAD = 64
WINDOW = 128
GRID_COLS = 64
EPSILON = 1e-06
ROPE_BASE = 10000.0
NEGATIVE = -1e30
LOG2E = math.log2(math.e)
LANES = 128
MESH = pl.DeviceIdType.MESH
f32 = jnp.float32
bf16 = jnp.bfloat16


def lanes_of(rows):
    return lax.broadcasted_iota(jnp.int32, (rows, LANES), 1)


def drain(ref, sem):
    pltpu.make_async_copy(ref, ref, sem).wait()


def swapped(u, lane):
    return jnp.where(lane % 32 < 16, pltpu.roll(u, LANES - 16, 1), pltpu.roll(u, 16, 1))


class Scores:
    def __init__(self, kv, ckv, q_ref, sample, row):
        self.kv, self.ckv, self.sample, self.row = kv, ckv, sample, row
        turned = q_ref[sample, pl.ds(row, WINDOW), :].astype(f32).T.astype(bf16)
        self.q = jnp.concatenate([turned[h * HEAD : (h + 1) * HEAD] for h in range(4)], axis=1)
        self.top = None

    def put(self, score, score_ref, at):
        rows = score.shape[0]
        score_ref[at : at + rows, :] = score
        top = jnp.max(score.reshape(rows // 8, 8, score.shape[1]), axis=0)
        self.top = top if self.top is None else jnp.maximum(self.top, top)

    def far(self, at, rows, score_ref):
        local = self.ckv.shape[2]
        keys = self.ckv[self.sample, at // local : (at + rows) // local].reshape(rows, LANES)
        self.put(jnp.dot(keys[:, :HEAD], self.q, preferred_element_type=f32), score_ref, at)

    def near(self, at, score_ref, offset):
        keys = self.kv[self.sample, pl.ds(pl.multiple_of(self.row + at, WINDOW), WINDOW), :]
        score = jnp.dot(keys[:, :HEAD], self.q, preferred_element_type=f32)
        if at != WINDOW:
            key = lax.broadcasted_iota(jnp.int32, score.shape, 0)
            query = lax.broadcasted_iota(jnp.int32, score.shape, 1) % WINDOW
            inside = key >= query if at == 0 else key <= query
            score = jnp.where(inside, score, NEGATIVE) + offset
        self.put(score, score_ref, at)


class Weights:
    def __init__(self, vt, limits, att, ctx, sample, row, score_ref, near_ref, top_ref):
        self.vt, self.att, self.ctx, self.sample, self.row, self.score_ref = vt, att, ctx, sample, row, score_ref
        self.near_ref = near_ref
        self.top = top_ref[0:1, :]
        self.lowered = self.top - limits[0:1, :]
        self.sink = jnp.exp2(limits[1:2, :] - self.top)
        self.total = jnp.zeros((vt.shape[1], 4 * WINDOW), f32)

    def piece(self, kind, at, rows):
        if kind == "far":
            score, top = self.score_ref[at : at + rows, :], self.lowered
            values = self.vt[self.sample, :, at : at + rows]
        else:
            score, top = self.near_ref[at : at + rows, :], self.top
            values = self.vt[self.sample, :, pl.ds(pl.multiple_of(self.ctx + self.row + at, WINDOW), rows)]
        weight = jnp.exp2(score - top).astype(bf16)
        self.total = self.total + jnp.dot(values, weight, preferred_element_type=f32)

    def done(self):
        out = self.total[16:] * (1.0 / (self.total[0:1] + self.sink))
        stacked = jnp.concatenate([out[:, h * WINDOW : (h + 1) * WINDOW] for h in range(4)], axis=0)
        self.att[self.sample, pl.ds(self.row, WINDOW), :] = stacked.T.astype(bf16)


def gated(by_v, wo_v, modr_v, sample, cols):
    owners = by_v.shape[0]
    rows = wo_v.shape[0] // owners
    total = jnp.zeros((by_v.shape[2], modr_v[0:1, cols].shape[1]), f32)
    for t in range(owners):
        total = total + jnp.dot(
            by_v[t, sample], wo_v[t * rows : (t + 1) * rows, cols], preferred_element_type=f32
        )
    return (total * modr_v[6 + sample : 7 + sample, cols]).astype(bf16)


def closing(first_v, by_v, wo_v, modr_v, out_hbm, last_v, sem):
    copies = [pltpu.make_async_copy(first_v, out_hbm.at[0], sem.at[0])]
    copies[0].start()
    wide = last_v.shape[1] // 4
    for n in range(4):
        cols = slice(n * wide, (n + 1) * wide)
        last_v[:, cols] = gated(by_v, wo_v, modr_v, 1, cols)
        copies.append(pltpu.make_async_copy(last_v.at[:, cols], out_hbm.at[1, :, cols], sem.at[1 + n]))
        copies[-1].start()
    for copy in copies:
        copy.wait()


def layer(
    sizes,
    x_hbm, context_hbm, condition_hbm, ctx_cond_hbm, gain_hbm, wsh_hbm, wsc_hbm, wga_hbm, wq_hbm, wk_hbm, wv_hbm, wo_hbm,
    sink_hbm, lift_hbm,
    out_v, by_v, wo_v, modr_v,
    condition, ctx_cond, gain, sink_ref, lift_ref, x_v, context_v, wm_v, wq_v, wt_v, wkv_v,
    active_v, part_v, rx_v, zsrc_v, rz_v, mod_v, mul_v, add_v,
    inv_v, cos_v, sin_v, q_v, kv_v, ckv_v, vt_v, limits_v, near_v, near_top_v, s0_v, s1_v, t0_v, t1_v, att_v,
    local_sem, stage_sem, ctx_sem, halo_send, halo_recv, wo_send, wo_recv, att_send, att_recv,
):
    nsp, nx, nt, nd = sizes
    nz = nsp // nx
    samples, tokens, width = x_v.shape
    chunk = tokens // nt
    ctx_local = context_v.shape[1]
    ctx = ctx_local * nsp
    sp = lax.axis_index("sp")
    tp = lax.axis_index("tp")
    dp = lax.axis_index("dp")
    xi = lax.rem(sp, nx)
    zi = lax.div(sp, nx)

    def place(sp_to=None, tp_to=None, dp_to=None):
        return {
            "sp": sp if sp_to is None else sp_to,
            "tp": tp if tp_to is None else tp_to,
            "dp": dp if dp_to is None else dp_to,
        }

    def remote(src, dst, send, recv, device):
        return pltpu.make_async_remote_copy(
            src_ref=src, dst_ref=dst, send_sem=send, recv_sem=recv, device_id=device, device_id_type=MESH
        )

    def x_peer(offset):
        return zi * nx + lax.rem(xi + offset, nx)

    def z_peer(offset):
        return lax.rem(zi + offset, nz) * nx + xi

    own_rows = wo_hbm.shape[0]
    half = own_rows // nd
    loads = [
        pltpu.make_async_copy(wsh_hbm, wm_v.at[0], local_sem.at[0]),
        pltpu.make_async_copy(wsc_hbm, wm_v.at[1], local_sem.at[1]),
        pltpu.make_async_copy(wga_hbm, wm_v.at[2], local_sem.at[2]),
        pltpu.make_async_copy(
            wo_hbm, wo_v.at[pl.ds(pl.multiple_of(tp * own_rows, own_rows), own_rows), :], local_sem.at[3]
        ),
        pltpu.make_async_copy(context_hbm, context_v, local_sem.at[4]),
        pltpu.make_async_copy(x_hbm, x_v, local_sem.at[5]),
        pltpu.make_async_copy(wk_hbm, wt_v.at[pl.ds(0, HEAD), :], local_sem.at[6]),
        pltpu.make_async_copy(wv_hbm, wt_v.at[pl.ds(HEAD, HEAD), :], local_sem.at[7]),
        pltpu.make_async_copy(wq_hbm, wq_v, local_sem.at[8]),
    ]
    small = [
        pltpu.make_async_copy(condition_hbm, condition, local_sem.at[9]),
        pltpu.make_async_copy(ctx_cond_hbm, ctx_cond, local_sem.at[10]),
        pltpu.make_async_copy(gain_hbm, gain, local_sem.at[11]),
        pltpu.make_async_copy(sink_hbm, sink_ref, local_sem.at[12]),
        pltpu.make_async_copy(lift_hbm, lift_ref, local_sem.at[13]),
    ]
    for load in small[:2] + loads[:3] + loads[6:8] + loads[3:5] + loads[8:] + small[2:] + loads[5:6]:
        load.start()

    barrier = pltpu.get_barrier_semaphore()

    def greet(device):
        pl.semaphore_signal(barrier, inc=1, device_id=device, device_id_type=MESH)

    for offset in range(1, nx):
        greet(place(sp_to=x_peer(offset)))
    for offset in range(1, nz):
        greet(place(sp_to=z_peer(offset)))
    for offset in range(1, nt):
        greet(place(tp_to=lax.rem(tp + offset, nt)))
    for offset in range(1, nd):
        greet(place(dp_to=lax.rem(dp + offset, nd)))

    active_v[...] = jnp.zeros_like(active_v)
    for load in small[:2]:
        load.wait()
    active_v[0:2, :] = condition[...].astype(f32)
    active_v[2:3, :] = ctx_cond[...].astype(f32)
    raw = active_v[...]
    active = (raw / (1.0 + jnp.exp(-raw))).astype(bf16)
    for load in loads[:3]:
        load.wait()
    vecs = [jnp.dot(active, wm_v[k], preferred_element_type=f32) for k in range(3)]
    for c in range(nx):
        cols = slice(c * LANES, (c + 1) * LANES)
        part_v[c, 0:3, :] = vecs[0][0:3, cols]
        part_v[c, 3:6, :] = vecs[1][0:3, cols]
        part_v[c, 6:8, :] = vecs[2][0:2, cols]

    pl.semaphore_wait(barrier, (nx - 1) + (nz - 1) + (nt - 1) + (nd - 1))

    for offset in range(1, nx):
        to = lax.rem(xi + offset, nx)
        remote(part_v.at[to], rx_v.at[offset - 1], stage_sem.at[0], stage_sem.at[1], place(sp_to=x_peer(offset))).start()

    loads[3].wait()

    def wo_rows(owner, core, start, count):
        return wo_v.at[pl.ds(pl.multiple_of(owner * own_rows + core * half + start, count), count), :]

    after = lax.rem(tp + 1, nt)
    before = lax.rem(tp + nt - 1, nt)
    across = lax.rem(tp + 2, nt)
    other = lax.rem(dp + 1, nd)
    quarter = half // 2

    def wo_copy(k, ref, device):
        return remote(ref, ref, wo_send.at[k], wo_recv.at[k], device)

    wo_sends = [
        wo_copy(0, wo_rows(tp, dp, 0, quarter), place(tp_to=after)),
        wo_copy(1, wo_rows(tp, dp, 0, quarter), place(tp_to=before)),
        wo_copy(2, wo_rows(tp, dp, quarter, quarter), place(tp_to=after)),
        wo_copy(3, wo_rows(tp, dp, quarter, quarter), place(tp_to=before)),
        wo_copy(4, wo_rows(before, dp, 0, quarter), place(tp_to=after)),
        wo_copy(5, wo_rows(after, dp, quarter, quarter), place(tp_to=before)),
        wo_copy(6, wo_rows(before, dp, 0, half), place(dp_to=other)),
        wo_copy(7, wo_rows(after, dp, 0, half), place(dp_to=other)),
        wo_copy(8, wo_rows(across, dp, 0, half), place(dp_to=other)),
    ]
    wo_sends[0].start()
    wo_sends[1].start()

    block = min(256, chunk)
    blocks = tokens // block

    def statistics(step):
        sample, start = step // blocks, pl.multiple_of(step % blocks * block, block)
        total = jnp.zeros((block, LANES), f32)
        for c in range(width // LANES):
            piece = x_v[sample, pl.ds(start, block), c * LANES : (c + 1) * LANES].astype(f32)
            total = total + piece * piece
        mean = jnp.sum(total, axis=1, keepdims=True) / width
        inv_v[sample, pl.ds(start, block), :] = jnp.broadcast_to(lax.rsqrt(mean + EPSILON), (block, LANES))

    def stats_loop(first, last):
        def run(step, carry):
            statistics(step)
            return carry

        lax.fori_loop(first, last, run, 0)

    all_blocks = samples * blocks
    loads[6].wait()
    loads[7].wait()
    wkv_v[...] = wt_v[...].T
    lane1 = lanes_of(8)
    frequency = jnp.exp((lane1[0:1] % 16).astype(f32) * (-math.log(ROPE_BASE) / 16.0))
    grid_rows = tokens // GRID_COLS
    table_rows = max(grid_rows, 8)
    row_pos = (sp * grid_rows + lax.broadcasted_iota(jnp.int32, (table_rows, LANES), 0)).astype(f32)
    col_pos = lax.broadcasted_iota(jnp.int32, (GRID_COLS, LANES), 0).astype(f32)
    row_cos, row_sin = jnp.cos(row_pos * frequency), jnp.sin(row_pos * frequency)
    col_cos, col_sin = jnp.cos(col_pos * frequency), jnp.sin(col_pos * frequency)
    lane64 = lanes_of(GRID_COLS)
    by_row = lane64 % HEAD < 32
    minus = lane64 % 32 < 16
    for t in range(grid_rows):
        rows = slice(t * GRID_COLS, (t + 1) * GRID_COLS)
        cos_v[rows, :] = jnp.where(by_row, row_cos[t : t + 1, :], col_cos)
        sine = jnp.where(by_row, row_sin[t : t + 1, :], col_sin)
        sin_v[rows, :] = jnp.where(minus, -sine, sine)

    drain(rx_v, stage_sem.at[1])
    quarter_sum = part_v[xi]
    for k in range(nx - 1):
        quarter_sum = quarter_sum + rx_v[k]
    zsrc_v[...] = quarter_sum

    for offset in range(1, nz):
        remote(zsrc_v, rz_v.at[offset - 1], stage_sem.at[2], stage_sem.at[3], place(sp_to=z_peer(offset))).start()

    loads[5].wait()
    stats_loop(0, all_blocks // 2)
    drain(rz_v, stage_sem.at[3])
    total = zsrc_v[...]
    for k in range(nz - 1):
        total = total + rz_v[k]
    here = tp * nx + xi
    mod_v[here] = total

    for dy in range(nt):
        for dx in range(nx):
            if dy or dx:
                remote(
                    mod_v.at[here], mod_v.at[here], stage_sem.at[4], stage_sem.at[5],
                    place(sp_to=x_peer(dx), tp_to=lax.rem(tp + dy, nt)),
                ).start()

    wo_sends[2].start()
    wo_sends[3].start()
    wo_sends[0].wait_recv()
    wo_sends[4].start()

    @pl.when(sp == 0)
    def _():
        kv_v[:, 0:WINDOW, :] = jnp.zeros((samples, WINDOW, LANES), bf16)

    @pl.when(sp == nsp - 1)
    def _():
        kv_v[:, WINDOW + tokens :, :] = jnp.zeros((samples, WINDOW, LANES), bf16)

    loads[4].wait()
    loads[8].wait()
    ctx_rows = samples * ctx_local
    ctx_wide = context_v[...].reshape(ctx_rows, width).astype(f32)
    ctx_inv = lax.rsqrt(jnp.mean(ctx_wide * ctx_wide, axis=1, keepdims=True) + EPSILON)
    ctx_unit = ctx_wide * ctx_inv

    stats_loop(all_blocks // 2, all_blocks)
    drain(mod_v.at[pl.ds(0, nt * nx - 1)], stage_sem.at[5])
    for k in range(nt * nx):
        modr_v[:, k * LANES : (k + 1) * LANES] = mod_v[k]
    small[2].wait()
    scaled = gain[...] * (1.0 + modr_v[3:6, :])
    for r in range(samples):
        mul_v[r, 0:1, :] = scaled[r : r + 1]
        add_v[r, 0:1, :] = modr_v[r : r + 1, :]

    ctx_hidden = (ctx_unit * scaled[2:3] + modr_v[2:3, :]).astype(bf16)
    ctx_pairs = jnp.dot(ctx_hidden, wkv_v[...], preferred_element_type=f32).astype(bf16)
    ckv_v[:, pl.ds(sp, 1)] = ctx_pairs.reshape(samples, 1, ctx_local, LANES)

    def ctx_rows_of(owner):
        return ckv_v.at[:, pl.ds(owner, 1)]

    def ctx_along_x(owner_z):
        rows = ctx_rows_of(owner_z * nx + xi)
        for offset in range(1, nx):
            remote(rows, rows, stage_sem.at[6], stage_sem.at[7], place(sp_to=x_peer(offset))).start()

    def ctx_along_z(offset):
        rows = ctx_rows_of(sp)
        return remote(rows, rows, ctx_sem.at[0, offset], ctx_sem.at[1, offset], place(sp_to=z_peer(offset)))

    far_z = [nz // 2]
    near_z = [offset for offset in range(1, nz) if min(offset, nz - offset) < min(3, nz // 2)]
    mid_z = [offset for offset in range(1, nz) if offset not in near_z + far_z]
    for offset in near_z + mid_z:
        ctx_along_z(offset).start()
    ctx_along_x(zi)
    own_pairs = ctx_rows_of(sp)
    for offset in far_z:
        ctx_along_z(offset).start()
        for dx in range(1, nx):
            to = lax.rem(zi + offset, nz) * nx + lax.rem(xi + dx, nx)
            remote(own_pairs, own_pairs, stage_sem.at[6], stage_sem.at[7], place(sp_to=to)).start()

    def pass_on(offsets):
        for offset in offsets:
            ctx_along_z(offset).wait_recv()
            ctx_along_x(lax.rem(zi + nz - offset, nz))

    lane = lanes_of(block)
    low = lane < HEAD

    assert blocks == 4 and samples == 2
    steps = 4
    deep = width // steps
    factor = HEAD ** (-0.5) * LOG2E

    def block_of(step):
        late, turn = step // 4, step % 4
        index = (1 - late) * (turn % 2) * (blocks - 1) + late * (1 + turn % 2)
        return turn // 2, pl.multiple_of(index * block, block)

    def store_values(pairs_t, sample, start):
        vt_v[sample, 16:, pl.ds(start, pairs_t.shape[1])] = pairs_t[HEAD:].astype(bf16)

    def project(step):
        sample, start = block_of(step)
        inverse = inv_v[sample, pl.ds(start, block), :]
        q_acc = jnp.zeros((block, 2 * LANES), f32)
        kv_acc = jnp.zeros((block, LANES), f32)
        for k in range(steps):
            hidden = []
            for c in range(deep // LANES):
                cols = slice(k * deep + c * LANES, k * deep + (c + 1) * LANES)
                wide = x_v[sample, pl.ds(start, block), cols].astype(f32)
                hidden.append((wide * inverse * mul_v[sample, 0:1, cols] + add_v[sample, 0:1, cols]).astype(bf16))
            hidden = jnp.concatenate(hidden, axis=1)
            q_acc = q_acc + jnp.dot(hidden, wq_v[k * deep : (k + 1) * deep, :], preferred_element_type=f32)
            kv_acc = kv_acc + jnp.dot(hidden, wkv_v[k * deep : (k + 1) * deep, :], preferred_element_type=f32)
        cosine = cos_v[pl.ds(start, block), :]
        sine = sin_v[pl.ds(start, block), :]
        turned = jnp.where(low, kv_acc * cosine + swapped(kv_acc, lane) * sine, kv_acc)
        kv_v[sample, pl.ds(pl.multiple_of(WINDOW + start, WINDOW), block), :] = turned.astype(bf16)
        store_values(turned.T, sample, pl.multiple_of(ctx + WINDOW + start, WINDOW))
        for pair in range(2):
            u = q_acc[:, pair * LANES : (pair + 1) * LANES]
            turned = (u * cosine + swapped(u, lane) * sine) * factor
            q_v[sample, pl.ds(start, block), pair * LANES : (pair + 1) * LANES] = turned.astype(bf16)

    send_right = remote(
        kv_v.at[:, pl.ds(tokens, WINDOW), :], kv_v.at[:, pl.ds(0, WINDOW), :], halo_send.at[0], halo_recv.at[0],
        place(sp_to=lax.rem(sp + 1, nsp)),
    )
    send_left = remote(
        kv_v.at[:, pl.ds(WINDOW, WINDOW), :], kv_v.at[:, pl.ds(WINDOW + tokens, WINDOW), :], halo_send.at[1],
        halo_recv.at[1], place(sp_to=lax.rem(sp + nsp - 1, nsp)),
    )

    def project_some(first, count):
        def run(group, carry):
            for member in range(count):
                project(first + count * group + member)
            return carry

        lax.fori_loop(0, 1, run, 0)

    project_some(0, 4)

    @pl.when(sp < nsp - 1)
    def _():
        send_right.start()

    @pl.when(sp > 0)
    def _():
        send_left.start()

    project_some(4, 2)
    pass_on(near_z)
    wo_sends[3].wait_recv()
    wo_sends[5].start()
    project_some(6, 2)
    pass_on(mid_z)

    assert nt == 4

    def destination(k):
        late = k // 2
        return lax.rem(tp + (1 - late) * (2 - k) + late * (9 - 3 * k), nt)

    def att_copy(step_k, sample):
        dest = destination(step_k)
        return remote(
            att_v.at[sample, pl.ds(pl.multiple_of(dest * chunk, chunk), chunk), :], by_v.at[tp, sample],
            att_send.at[step_k, sample], att_recv.at[step_k, sample], place(tp_to=dest),
        )

    for load, ref, line in ((small[4], lift_ref, 0), (small[3], sink_ref, 1)):
        load.wait()
        for h in range(4):
            limits_v[line : line + 1, h * WINDOW : (h + 1) * WINDOW] = jnp.broadcast_to(
                ref[0:1, h : h + 1] * LOG2E, (1, WINDOW)
            )
    subs = chunk // WINDOW
    deep_keys = min(256, ctx)
    pieces = [("far", c * deep_keys, deep_keys) for c in range(ctx // deep_keys)]
    pieces += [("near", c * WINDOW, WINDOW) for c in range(3)]
    buffers = ((s0_v, t0_v), (s1_v, t1_v))

    def rows_of(step, sub):
        k, sample = step // samples, step % samples
        dest = destination(k)
        return sample, pl.multiple_of(dest * chunk + sub * WINDOW, WINDOW)

    def near_scores(sample, dest):
        place_of = dest * samples + sample
        for sub in range(subs):
            row = pl.multiple_of(dest * chunk + sub * WINDOW, WINDOW)
            left_off = jnp.where((sp == 0) & (row == 0), NEGATIVE, 0.0)
            right_off = jnp.where((sp == nsp - 1) & (row == tokens - WINDOW), NEGATIVE, 0.0)
            score = Scores(kv_v, ckv_v, q_v, sample, row)
            for at, offset in ((0, left_off), (WINDOW, 0.0), (2 * WINDOW, right_off)):
                score.near(at, near_v.at[place_of, sub], offset)
            near_top_v[place_of, sub] = score.top

    def near_of(step):
        k, sample = step // samples, step % samples
        return destination(k) * samples + sample

    def near_pair(first, apart):
        def run(turn, carry):
            for sample in range(samples):
                near_scores(sample, first + apart * turn)
            return carry

        lax.fori_loop(0, 2, run, 0)

    near_pair(1, 1)

    @pl.when(sp > 0)
    def _():
        send_right.wait_recv()

    @pl.when(sp < nsp - 1)
    def _():
        send_left.wait_recv()

    for sample in range(samples):
        store_values(kv_v[sample, :WINDOW].astype(f32).T, sample, ctx)
        store_values(kv_v[sample, WINDOW + tokens :].astype(f32).T, sample, ctx + WINDOW + tokens)
        vt_v[sample, :16, :] = jnp.ones((16, ctx + tokens + 2 * WINDOW), bf16)
    near_pair(0, nt - 1)

    for offset in far_z:
        ctx_along_z(offset).wait_recv()
    drain(ckv_v.at[:, pl.ds(0, nz * (nx - 1))], stage_sem.at[7])
    for sample in range(samples):
        store_values(ckv_v[sample].reshape(ctx, LANES).astype(f32).T, sample, 0)


    def scores(step, sub):
        sample, row = rows_of(step, sub)
        return Scores(kv_v, ckv_v, q_v, sample, row)

    def weights(step, buffer, sub):
        sample, row = rows_of(step, sub)
        score_ref, top_ref = buffer
        return Weights(
            vt_v, limits_v, att_v, ctx, sample, row, score_ref.at[sub], near_v.at[near_of(step), sub], top_ref.at[sub]
        )

    def both(now, later, step, buffer):
        for kind, at, rows in pieces:
            for sub in range(subs):
                if now:
                    now[sub].piece(kind, at, rows)
                if later and kind == "far":
                    later[sub].far(at, rows, buffer[0].at[sub])
        for sub in range(subs):
            if later:
                far = jnp.max(later[sub].top, axis=0, keepdims=True) + limits_v[0:1, :]
                near = jnp.max(near_top_v[near_of(step), sub], axis=0, keepdims=True)
                buffer[1][sub, 0:1, :] = jnp.maximum(jnp.maximum(far, near), limits_v[1:2, :])
            if now:
                now[sub].done()

    both(None, [scores(0, sub) for sub in range(subs)], 0, buffers[0])
    turns = nt * samples

    def chunk_step(step, carry):
        for parity in range(2):

            @pl.when(step % 2 == parity)
            def _():
                both(
                    [weights(step, buffers[parity], sub) for sub in range(subs)],
                    [scores(step + 1, sub) for sub in range(subs)],
                    step + 1,
                    buffers[1 - parity],
                )

        k, sample = step // samples, step % samples

        @pl.when(k < nt - 1)
        def _():
            att_copy(k, sample).start()

        @pl.when(step == 1)
        def _():
            wo_sends[1].wait_recv()
            wo_sends[2].wait_recv()
            wo_sends[6].start()
            wo_sends[7].start()

        @pl.when(step == 3)
        def _():
            wo_sends[4].wait_recv()
            wo_sends[5].wait_recv()
            wo_sends[8].start()

        return carry

    lax.fori_loop(0, turns - 1, chunk_step, 0)
    own = pl.ds(pl.multiple_of(tp * chunk, chunk), chunk)
    by_v[tp, 0] = att_v[0, own, :]
    for k in (6, 7, 8):
        wo_sends[k].wait_recv()
    for k in range(nt - 1):
        att_copy(k, 0).wait_recv()
    both([weights(turns - 1, buffers[(turns - 1) % 2], sub) for sub in range(subs)], None, None, None)
    out_v[...] = gated(by_v, wo_v, modr_v, 0, slice(0, width))
    by_v[tp, 1] = att_v[1, own, :]
    for k in range(nt - 1):
        att_copy(k, 1).wait_recv()

    drain(rx_v, stage_sem.at[0])
    drain(rz_v, stage_sem.at[2])
    drain(mod_v.at[pl.ds(0, nt * nx - 1)], stage_sem.at[4])
    drain(ckv_v.at[:, pl.ds(0, nz * (nx - 1))], stage_sem.at[6])
    for offset in range(1, nz):
        ctx_along_z(offset).wait_send()
    for copy in wo_sends:
        copy.wait_send()

    @pl.when(sp < nsp - 1)
    def _():
        send_right.wait_send()

    @pl.when(sp > 0)
    def _():
        send_left.wait_send()

    for k in range(nt - 1):
        for sample in range(samples):
            att_copy(k, sample).wait_send()


def shards(
    sizes, latent, context, condition, ctx_cond, norm_gain, w_shift, w_scale, w_gate, w_query, w_key, w_value, w_out,
    sink_logit, ctx_lift,
):
    nsp, nx, nt, nd = sizes
    nz = nsp // nx
    samples, tokens, width = latent.shape
    ctx_local = context.shape[1]
    ctx = ctx_local * nsp
    feats = condition.shape[1]
    cols = w_shift.shape[1]
    chunk = tokens // nt
    keys = ctx + tokens + 2 * WINDOW
    own_rows = w_out.shape[0]
    anywhere = pl.BlockSpec(memory_space=pltpu.HBM)
    vmem = pl.BlockSpec(memory_space=pltpu.VMEM)
    dma = pltpu.SemaphoreType.DMA
    kept = pl.pallas_call(
        functools.partial(layer, sizes),
        out_shape=(
            pltpu.VMEM((chunk, width), bf16),
            pltpu.VMEM((nt, samples, chunk, 2 * LANES), bf16),
            pltpu.VMEM((own_rows * nt, width), bf16),
            pltpu.VMEM((8, width), f32),
        ),
        in_specs=[anywhere] * 14,
        out_specs=(vmem,) * 4,
        scratch_shapes=[
            pltpu.VMEM((samples, feats), bf16),
            pltpu.VMEM((1, feats), bf16),
            pltpu.VMEM((1, width), f32),
            pltpu.VMEM((1, 4), f32),
            pltpu.VMEM((1, 4), f32),
            pltpu.VMEM((samples, tokens, width), bf16),
            pltpu.VMEM((samples, ctx_local, width), bf16),
            pltpu.VMEM((3, feats, cols), bf16),
            pltpu.VMEM((width, 4 * HEAD), bf16),
            pltpu.VMEM((LANES, width), bf16),
            pltpu.VMEM((width, LANES), bf16),
            pltpu.VMEM((16, feats), f32),
            pltpu.VMEM((nx, 8, LANES), f32),
            pltpu.VMEM((nx - 1, 8, LANES), f32),
            pltpu.VMEM((8, LANES), f32),
            pltpu.VMEM((nz - 1, 8, LANES), f32),
            pltpu.VMEM((nt * nx, 8, LANES), f32),
            pltpu.VMEM((samples, 8, width), f32),
            pltpu.VMEM((samples, 8, width), f32),
            pltpu.VMEM((samples, tokens, LANES), f32),
            pltpu.VMEM((tokens, LANES), f32),
            pltpu.VMEM((tokens, LANES), f32),
            pltpu.VMEM((samples, tokens, 4 * HEAD), bf16),
            pltpu.VMEM((samples, tokens + 2 * WINDOW, LANES), bf16),
            pltpu.VMEM((samples, nsp, ctx_local, LANES), bf16),
            pltpu.VMEM((samples, HEAD + 16, keys), bf16),
            pltpu.VMEM((8, 4 * WINDOW), f32),
            pltpu.VMEM((nt * samples, chunk // WINDOW, 3 * WINDOW, 4 * WINDOW), f32),
            pltpu.VMEM((nt * samples, chunk // WINDOW, 8, 4 * WINDOW), f32),
            pltpu.VMEM((chunk // WINDOW, ctx, 4 * WINDOW), f32),
            pltpu.VMEM((chunk // WINDOW, ctx, 4 * WINDOW), f32),
            pltpu.VMEM((chunk // WINDOW, 8, 4 * WINDOW), f32),
            pltpu.VMEM((chunk // WINDOW, 8, 4 * WINDOW), f32),
            pltpu.VMEM((samples, tokens, 2 * LANES), bf16),
            dma((14,)),
            dma((8,)),
            dma((2, nz)),
            dma((2,)),
            dma((2,)),
            dma((9,)),
            dma((9,)),
            dma((nt - 1, samples)),
            dma((nt - 1, samples)),
        ],
        compiler_params=pltpu.CompilerParams(
            collective_id=0, has_side_effects=True, vmem_limit_bytes=56 * 1024 * 1024
        ),
        name="layer",
    )(
        latent, context, condition, ctx_cond.reshape(1, feats), norm_gain.reshape(1, width), w_shift, w_scale, w_gate,
        w_query, w_key.T, w_value.T, w_out, sink_logit.reshape(1, 4), ctx_lift.reshape(1, 4),
    )
    return pl.pallas_call(
        closing,
        out_shape=jax.ShapeDtypeStruct((samples, chunk, width), bf16),
        in_specs=[vmem] * 4,
        out_specs=anywhere,
        scratch_shapes=[pltpu.VMEM((chunk, width), bf16), dma((5,))],
        compiler_params=pltpu.CompilerParams(vmem_limit_bytes=16 * 1024 * 1024),
        name="closing",
    )(*kept)


def solution(mesh):
    nsp, nt, nd = mesh.shape["sp"], mesh.shape["tp"], mesh.shape["dp"]
    sizes = (nsp, 4 if nsp > 4 else 2, nt, nd)
    return jax.shard_map(
        functools.partial(shards, sizes),
        mesh=mesh,
        in_specs=(
            P("dp", "sp", None),
            P("dp", "sp", None),
            P("dp", "sp"),
            P("sp"),
            P(),
            P("sp", "tp"),
            P("sp", "tp"),
            P("sp", "tp"),
            P(None, "tp"),
            P(None, "tp"),
            P(None, "tp"),
            P("tp", None),
            P("tp"),
            P("tp"),
        ),
        out_specs=P("dp", ("sp", "tp"), None),
        check_vma=False,
    )
```
